256 devices in a mesh: sp: 32 (over z, x), tp: 4 (over y), dp: 2 (over core).
Axes of the slice: x: 4, y: 4, z: 8, core: 2. Of those that a mesh axis runs over, the one named last changes fastest.
Arguments:
- latent: bfloat16 [2, 6144, 2048], P('dp', 'sp'), may hold values from -6 to 6
- cond: bfloat16 [2, 2048], P('dp', 'sp'), may hold values from -6 to 6
- context: bfloat16 [2, 256, 2048], P('dp', 'sp'), may hold values from -6 to 6
- ctx_cond: bfloat16 [2048], P('sp'), may hold values from -6 to 6
- w_mod: bfloat16 [2048, 6144], P('sp', 'tp'), may hold values from -0.125 to 0.125
- norm_gain: bfloat16 [2048], replicated, may hold values from 0.099609375 to 1.8984375
- w_query: bfloat16 [2048, 1024], P(None, 'tp'), may hold values from -0.125 to 0.125
- w_key: bfloat16 [2048, 1024], P(None, 'tp'), may hold values from -0.125 to 0.125
- w_value: bfloat16 [2048, 1024], P(None, 'tp'), may hold values from -0.125 to 0.125
- w_outgate: bfloat16 [2048, 1024], P(None, 'tp'), may hold values from -0.125 to 0.125
- w_decay: bfloat16 [2048, 2, 8], P(None, None, 'tp'), may hold values from -0.125 to 0.125
- w_beta: bfloat16 [2048, 2, 8], P(None, None, 'tp'), may hold values from -0.125 to 0.125
- decay_rate: float32 [2, 8], P(None, 'tp'), may hold values from 8.138021e-06 to 0.0333333333
- decay_bias: float32 [2, 8], P(None, 'tp'), may hold values from -3 to 3
- extra_decay: float32 [2, 2, 8, 6144], P('dp', None, 'tp', 'sp'), may hold values from -0.7000977 to -1.6276042e-05
- out_gain: bfloat16 [128], replicated, may hold values from 0.099609375 to 1.8984375
- w_out: bfloat16 [1024, 2048], replicated, may hold values from -0.1875 to 0.1875
Outputs:
- mixed_out: bfloat16 [2, 6144, 2048], P('dp', ('sp', 'tp'))
The draws below stay inside these ranges and needn't reach their ends.
All inputs are finite; a program needn't handle non-finite values.
Results may differ from the reference program's by a relative error of at most 0.0067.
Values may be sent and summed in bfloat16 or wider, within the bound.
No kernel may reach another device: no remote copies, remote signals or barrier semaphores. Data moves between devices by JAX's collectives and lax.ppermute only.
A program may use at most 128 MiB of HBM per device.

```python
import math
import jax
import jax.numpy as jnp
from jax import lax

D = 2048
HEADS = 8
HEAD = 128
BLOCK = 64
TOK_DEV = 192
SAMPLES = 2
LATENT_TOKENS = 6144
CONTEXT = 256


def draw_decay_rate(key, part):
    pick_key, fast_key, middle_key, slow_key = jax.random.split(key, 4)
    fast_share = 0.2
    middle_share = 0.3
    picked = jax.random.uniform(pick_key, (2, HEADS), jnp.float32)
    fast_rate = jnp.exp(jax.random.uniform(fast_key, (2, HEADS), jnp.float32, math.log(1.0 / 50.0), math.log(1.0 / 30.0)))
    middle_rate = jnp.exp(jax.random.uniform(middle_key, (2, HEADS), jnp.float32, math.log(0.001), math.log(0.01)))
    slow_rate = jnp.exp(jax.random.uniform(slow_key, (2, HEADS), jnp.float32, math.log(0.05 / LATENT_TOKENS), math.log(0.3 / LATENT_TOKENS)))
    return jnp.where(picked < fast_share, fast_rate, jnp.where(picked < fast_share + middle_share, middle_rate, slow_rate))


def draw_extra_decay(key, part):
    rate_key, place_key, depth_key = jax.random.split(key, 3)
    span_count = LATENT_TOKENS // TOK_DEV
    block_rates = jnp.exp(jax.random.uniform(rate_key, (SAMPLES, 2, HEADS, span_count), jnp.float32, math.log(0.1 / LATENT_TOKENS), math.log(0.6 / LATENT_TOKENS)))
    steady_state = -jnp.repeat(block_rates, TOK_DEV, axis=-1)
    third_len = LATENT_TOKENS // 3
    offsets = jax.random.randint(place_key, (SAMPLES, 2, HEADS, 3), 0, third_len)
    token_places = offsets + third_len * jnp.arange(3)
    depth_values = jnp.log(jax.random.uniform(depth_key, (SAMPLES, 2, HEADS, 3), jnp.float32, 0.5, 0.8))
    impulse_matches = (jnp.arange(LATENT_TOKENS)[None, None, None, None, :] == token_places[..., None]).astype(jnp.float32)
    return steady_state + jnp.sum(impulse_matches * depth_values[..., None], axis=-2)


def shard_levels(rng, dims, cuts, least, top_value):
    def one(axis_at, blocks):
        steps = jax.random.uniform(jax.random.fold_in(jax.random.fold_in(rng, 6), axis_at), (blocks,), jnp.float32, least / len(cuts), top_value / len(cuts))
        return jnp.repeat(jnp.exp(steps), dims[axis_at] // blocks).reshape((-1,) + (1,) * (len(dims) - axis_at - 1))

    factor_of = one(*cuts[0])
    for cut in cuts[1:]:
        factor_of = factor_of * one(*cut)
    return factor_of


def centred(rng, extent, deviation, most, cuts=(), kind=jnp.bfloat16):
    entries = deviation * jax.random.normal(rng, extent, jnp.float32)
    if cuts:
        entries = entries * shard_levels(rng, extent, cuts, -0.22, 0.18)
    return jnp.clip(entries, -most, most).astype(kind)


def setup_inputs(seed: int = 0) -> dict:
    seeds = jax.random.split(jax.random.key(seed), 18)
    return {
        "latent": centred(seeds[0], (SAMPLES, LATENT_TOKENS, D), 1.0, 6.0, ((0, 2), (1, 32))),
        "cond": centred(seeds[1], (SAMPLES, D), 1.0, 6.0, ((0, 2), (1, 32))),
        "context": centred(seeds[2], (SAMPLES, CONTEXT, D), 1.0, 6.0, ((0, 2), (1, 32))),
        "ctx_cond": centred(seeds[3], (D,), 1.0, 6.0, ((0, 32),)),
        "w_mod": centred(seeds[4], (D, 3 * D), D ** -0.5, 0.125, ((0, 32), (1, 4))),
        "norm_gain": jnp.clip(1.0 + 0.18 * jax.random.normal(seeds[5], (D,), jnp.float32), 0.099609375, 1.8984375).astype(jnp.bfloat16),
        "w_query": centred(seeds[6], (D, HEADS * HEAD), D ** -0.5, 0.125, ((1, 4),)),
        "w_key": centred(seeds[7], (D, HEADS * HEAD), D ** -0.5, 0.125, ((1, 4),)),
        "w_value": centred(seeds[8], (D, HEADS * HEAD), D ** -0.5, 0.125, ((1, 4),)),
        "w_outgate": centred(seeds[9], (D, HEADS * HEAD), D ** -0.5, 0.125, ((1, 4),)),
        "w_decay": centred(seeds[10], (D, 2, HEADS), D ** -0.5, 0.125, ((2, 4),)),
        "w_beta": centred(seeds[11], (D, 2, HEADS), D ** -0.5, 0.125, ((2, 4),)),
        "decay_rate": draw_decay_rate(jax.random.fold_in(seeds[17], 71), 0),
        "decay_bias": centred(seeds[13], (2, HEADS), 1.0, 3.0, ((1, 4),), jnp.float32),
        "extra_decay": draw_extra_decay(jax.random.fold_in(seeds[17], 71), 0),
        "out_gain": jnp.clip(1.0 + 0.18 * jax.random.normal(seeds[15], (HEAD,), jnp.float32), 0.099609375, 1.8984375).astype(jnp.bfloat16),
        "w_out": centred(seeds[16], (HEADS * HEAD, D), (HEADS * HEAD) ** -0.5, 0.1875),
    }


norm_eps = 1e-06
beta_scale = 30.0

def contract_product(einsum_form, left_op, right_op):
    return jnp.einsum(einsum_form, left_op, right_op, precision=lax.Precision.HIGHEST)

def modulate(rows_in, gain_vec, scale_row, shift_row):
    values = rows_in.astype(jnp.float32)
    normed = values * lax.rsqrt(lax.optimization_barrier(jnp.mean(values * values, axis=-1, keepdims=True)) + norm_eps)
    return (normed * gain_vec.astype(jnp.float32) * (1.0 + scale_row) + shift_row).astype(jnp.bfloat16)

def unit_normal(values):
    return values * lax.rsqrt(lax.optimization_barrier(jnp.sum(values * values, axis=-1, keepdims=True)) + norm_eps)

def head_view(raw_proj, head_count):
    return raw_proj.astype(jnp.float32).reshape(raw_proj.shape[0], head_count, -1)

def split_inputs(raw_proj, head_count, inner_width):
    row_count = raw_proj.shape[0]
    key_rows = unit_normal(jax.nn.silu(head_view(raw_proj[:, :inner_width], head_count)))
    value_rows = jax.nn.silu(head_view(raw_proj[:, inner_width:2 * inner_width], head_count))
    decay_raw = raw_proj[:, 2 * inner_width:2 * inner_width + 2 * head_count].astype(jnp.float32)
    beta_raw = raw_proj[:, 2 * inner_width + 2 * head_count:].astype(jnp.float32)
    return (key_rows, value_rows, decay_raw.reshape(row_count, 2, head_count), beta_raw.reshape(row_count, 2, head_count))

def orient(values, direction):
    if direction:
        return values[::-1]
    return values

def to_blocks(values, block_width):
    block_count = values.shape[0] // block_width
    shaped = values.reshape((block_count, block_width) + values.shape[1:])
    return jnp.moveaxis(shaped, 2, 1)

def unit_inverse(lowpart, block_width):
    positions = jnp.arange(block_width)
    result = jnp.broadcast_to(jnp.eye(block_width, dtype=jnp.float32), lowpart.shape)
    for level_index in range((block_width - 1).bit_length()):
        half_width = 1 << level_index
        same_pair = positions[:, None] // (2 * half_width) == positions[None, :] // (2 * half_width)
        lower_half = positions[:, None] // half_width % 2 == 1
        upper_half = positions[None, :] // half_width % 2 == 0
        coupling = jnp.where(same_pair & lower_half & upper_half, lowpart, 0.0)
        result = result - contract_product('nhij,nhjk->nhik', result, contract_product('nhij,nhjk->nhik', coupling, result))
    return result

def block_terms(key_rows, value_rows, log_decay, beta_rows, block_width):
    key_blocks = to_blocks(key_rows, block_width)
    value_blocks = to_blocks(value_rows, block_width)
    cumulative = jnp.cumsum(to_blocks(log_decay, block_width), axis=-1)
    beta_blocks = to_blocks(beta_rows, block_width)
    positions = jnp.arange(block_width)
    lower_mask = positions[:, None] >= positions[None, :]
    strict = positions[:, None] > positions[None, :]
    spread = cumulative[..., :, None] - cumulative[..., None, :]
    weights = jnp.where(lower_mask, jnp.exp(jnp.where(lower_mask, spread, 0.0)), 0.0)
    scaled = key_blocks * beta_blocks[..., None]
    lowpart = jnp.where(strict, contract_product('nhid,nhjd->nhij', scaled, key_blocks) * weights, 0.0)
    inverse = unit_inverse(lowpart, block_width)
    state_update = contract_product('nhij,nhjd->nhid', inverse, value_blocks * beta_blocks[..., None])
    erased_state = contract_product('nhij,nhjd->nhid', inverse, scaled * jnp.exp(cumulative)[..., None])
    final_log_decay = cumulative[..., -1]
    decayed_keys = key_blocks * jnp.exp(final_log_decay[..., None] - cumulative)[..., None]
    return ((state_update, erased_state, decayed_keys, final_log_decay), (key_blocks, cumulative, weights))

def query_terms(queries, extras):
    key_blocks, cumulative, weights = extras
    query_blocks = to_blocks(queries, key_blocks.shape[2])
    query_decayed = query_blocks * jnp.exp(cumulative)[..., None]
    query_keys = contract_product('nhid,nhjd->nhij', query_blocks, key_blocks) * weights
    return (query_decayed, query_keys)

def direction_terms(key_rows, value_rows, decay_raw, beta_raw, decay_rate, decay_bias, direction, added, block_width):
    log_decay = -decay_rate[direction] * jax.nn.softplus(decay_raw[:, direction] + decay_bias[direction]) + added
    beta_rows = jax.nn.sigmoid(beta_raw[:, direction]) * (beta_scale * decay_rate[direction])
    return block_terms(orient(key_rows, direction), orient(value_rows, direction), orient(log_decay, direction), orient(beta_rows, direction), block_width)

def carry_state(state_now, parts):

    def advance(carried_state, inputs):
        state_update, erased_state, decayed_keys, final_log_decay = inputs
        new_value_rows = state_update - contract_product('tze,tem->tzm', erased_state, carried_state)
        carried_state = carried_state * jnp.exp(final_log_decay)[:, None, None] + contract_product('rbz,rbi->rzi', decayed_keys, new_value_rows)
        return (carried_state, None)
    return lax.scan(advance, state_now, parts)[0]

def read_out(state_now, parts, query_decayed, query_keys):

    def advance(carried_state, inputs):
        state_update, erased_state, decayed_keys, final_log_decay, query_tile, query_matrix = inputs
        new_value_rows = state_update - contract_product('tze,tem->tzm', erased_state, carried_state)
        state_readout = contract_product('tze,tem->tzm', query_tile, carried_state) + contract_product('bgd,bdc->bgc', query_matrix, new_value_rows)
        carried_state = carried_state * jnp.exp(final_log_decay)[:, None, None] + contract_product('rbz,rbi->rzi', decayed_keys, new_value_rows)
        return (carried_state, state_readout)
    readouts = lax.scan(advance, state_now, parts + (query_decayed, query_keys))[1]
    block_count, head_count, block_width, value_width = readouts.shape
    return jnp.moveaxis(readouts, 1, 2).reshape(block_count * block_width, head_count, value_width)

def reference(latent, cond, context, ctx_cond, w_mod, norm_gain, w_query, w_key, w_value, w_outgate, w_decay, w_beta, decay_rate, decay_bias, extra_decay, out_gain, w_out):
    inner_width = HEADS * HEAD
    cond_all = jnp.concatenate([cond, ctx_cond[None, :]], axis=0)
    cond_rows = jax.nn.silu(cond_all.astype(jnp.float32)).astype(jnp.bfloat16)
    modulation = jnp.dot(cond_rows, w_mod, preferred_element_type=jnp.float32)
    shift_rows = modulation[:, :D]
    scale_rows = modulation[:, D:2 * D]
    gate_rows = modulation[:, 2 * D:]
    ctx_joined = jnp.concatenate([w_key, w_value, w_decay.reshape(D, 2 * HEADS), w_beta.reshape(D, 2 * HEADS)], axis=1)
    lat_joined = jnp.concatenate([w_query, w_outgate, ctx_joined], axis=1)
    zero_state = jnp.zeros((HEADS, HEAD, HEAD), jnp.float32)
    ctx_block = min(BLOCK, CONTEXT)
    results = []
    for sample in range(SAMPLES):
        ctx_in = modulate(context[sample], norm_gain, scale_rows[SAMPLES], shift_rows[SAMPLES])
        ctx_proj = jnp.dot(ctx_in, ctx_joined, preferred_element_type=jnp.float32).astype(jnp.bfloat16)
        lat_in = modulate(latent[sample], norm_gain, scale_rows[sample], shift_rows[sample])
        lat_proj = jnp.dot(lat_in, lat_joined, preferred_element_type=jnp.float32).astype(jnp.bfloat16)
        queries = unit_normal(jax.nn.silu(head_view(lat_proj[:, :inner_width], HEADS))) * HEAD ** (-0.5)
        outgate = lat_proj[:, inner_width:2 * inner_width]
        ctx_inputs = split_inputs(ctx_proj, HEADS, inner_width)
        lat_inputs = split_inputs(lat_proj[:, 2 * inner_width:], HEADS, inner_width)
        summed_out = jnp.zeros((LATENT_TOKENS, HEADS, HEAD), jnp.float32)
        for direction in range(2):
            ctx_parts = direction_terms(*ctx_inputs, decay_rate, decay_bias, direction, 0.0, ctx_block)[0]
            ctx_state = carry_state(zero_state, ctx_parts)
            lat_parts, extras = direction_terms(*lat_inputs, decay_rate, decay_bias, direction, extra_decay[sample, direction].T, BLOCK)
            query_decayed, query_keys = query_terms(orient(queries, direction), extras)
            summed_out = summed_out + orient(read_out(ctx_state, lat_parts, query_decayed, query_keys), direction)
        normed = summed_out * lax.rsqrt(lax.optimization_barrier(jnp.mean(summed_out * summed_out, axis=-1, keepdims=True)) + norm_eps)
        normed = normed * out_gain.astype(jnp.float32)
        gated = (normed * jax.nn.silu(head_view(outgate, HEADS))).reshape(LATENT_TOKENS, inner_width).astype(jnp.bfloat16)
        mixed_rows = jnp.dot(gated, w_out, preferred_element_type=jnp.float32)
        results.append((latent[sample].astype(jnp.float32) + gate_rows[sample] * mixed_rows).astype(jnp.bfloat16))
    return jnp.stack(results)
```

```python
import functools

import jax
import jax.numpy as jnp
from jax import lax
from jax.experimental import pallas as pl
from jax.experimental.pallas import tpu as pltpu
from jax.sharding import Mesh
from jax.sharding import PartitionSpec as P

D = 2048
HEAD = 128
LANES = 128
NORM_EPS = 1e-06
BETA_SCALE = 30.0

SPAN = 192
CTX_OWN = 8
ROWS = 208
CHUNK = 256
CHUNKS = 3
ROW_OF_X = 4 * SPAN

K_AT, V_AT, Q_AT, G_AT, S_AT, X_ROWS = 0, 208, 416, 608, 704, 720
C_AT, D_AT, Z_ROWS = 128, 160, 192

F32 = jnp.float32
BF16 = jnp.bfloat16


def dot(a, b, dims=((1,), (0,))):
    return lax.dot_general(a, b, (dims, ((), ())), preferred_element_type=F32)


def silu(v):
    return v / (1.0 + jnp.exp(-v))


def rounded(v):
    return v.astype(BF16).astype(F32)


def split_in_two(v):
    high = v.astype(BF16)
    return high.astype(F32), v - high.astype(F32)


def iota(shape, dim):
    return lax.broadcasted_iota(jnp.int32, shape, dim)


def partial_modulation(cond, ctx_cond, w_mod, out, rows):
    first = iota((8, cond.shape[1]), 0) == 0
    values = jnp.where(first, cond[...].astype(F32), ctx_cond[...].astype(F32))
    product = dot(silu(values).astype(BF16), w_mod[...])
    for r in range(2):
        for c in range(12):
            rows[r * 12 + c : r * 12 + c + 1, :] = product[r : r + 1, c * LANES : (c + 1) * LANES]
    value = rows[...].astype(BF16)
    for k in range(out.shape[0]):
        out[k] = value


def sum_and_spread(parts, out):
    total = parts[0].astype(F32)
    for k in range(1, parts.shape[0]):
        total = total + parts[k].astype(F32)
    value = total.astype(BF16)
    for k in range(out.shape[0]):
        out[k] = value


def modulated(values, gain, mods, which):
    scale = lax.rsqrt(jnp.mean(values * values, axis=-1, keepdims=True) + NORM_EPS)

    def row(block):
        at = (block // 12) * 24 + which * 12 + block % 12
        return mods[at : at + 1, :]

    out = []
    for j in range(D // LANES):
        cols = slice(j * LANES, (j + 1) * LANES)
        factor = gain[:, cols].astype(F32) * (1.0 + row(16 + j))
        out.append((values[:, cols] * scale * factor + row(j)).astype(BF16))
    return out


def project(
    parts, latent, context, gain, w_query, w_key, w_value, w_gate, w_small, rate, bias, extra,
    out, gate_out, mods, rows_in,
):
    for y in range(4):
        total = parts[y].astype(F32)
        for x in range(1, 4):
            total = total + parts[4 * x + y].astype(F32)
        mods[24 * y : 24 * y + 24, :] = total
    for j in range(16):
        block = 32 + j
        at = (block // 12) * 24 + block % 12
        gate_out[j : j + 1, :] = mods[at : at + 1, :]
    for g in range(0, SPAN, 64):
        for j, tile in enumerate(modulated(latent[g : g + 64, :].astype(F32), gain, mods, 0)):
            rows_in[g : g + 64, j * LANES : (j + 1) * LANES] = tile
    ctx_values = jnp.concatenate(
        [context[...].astype(F32), jnp.zeros((ROWS - SPAN - CTX_OWN, D), F32)], axis=0
    )
    for j, tile in enumerate(modulated(ctx_values, gain, mods, 1)):
        rows_in[SPAN:ROWS, j * LANES : (j + 1) * LANES] = tile
    inputs = rows_in[...]

    def heads(values):
        return [values[:, h * HEAD : (h + 1) * HEAD] for h in range(2)]

    small = rounded(dot(w_small[...], inputs, ((1,), (1,))))
    decay_raw, beta_raw = small[:4], small[4:]
    pre = decay_raw + bias[...]
    soft = jnp.maximum(pre, 0.0) + jnp.log1p(jnp.exp(-jnp.abs(pre)))
    added = jnp.concatenate([extra[...], jnp.zeros((4, ROWS - SPAN), F32)], axis=1)
    log_decay = -rate[...] * soft + added
    beta = BETA_SCALE * rate[...] / (1.0 + jnp.exp(-beta_raw))
    pad = jnp.zeros((4, 256 - ROWS), F32)
    g_high, g_low = split_in_two(jnp.concatenate([log_decay, pad], axis=1))
    b_high, b_low = split_in_two(jnp.concatenate([beta, pad], axis=1))

    def unit(v):
        return v * lax.rsqrt(jnp.sum(v * v, axis=-1, keepdims=True) + NORM_EPS)

    keys = heads(silu(rounded(dot(inputs, w_key[...]))))
    values = heads(silu(rounded(dot(inputs, w_value[...]))))
    queries = heads(silu(rounded(dot(inputs[:SPAN], w_query[...]))))
    gates = heads(silu(rounded(dot(inputs[:SPAN], w_gate[...]))))
    low_lanes = iota((24, LANES), 1) < 64
    for h in range(2):
        key = unit(keys[h]).astype(BF16)
        value = values[h].astype(BF16)
        query = (unit(queries[h]) * HEAD**-0.5).astype(BF16)
        for d in range(2):
            peer = 2 * h + d
            out[peer, K_AT:V_AT, :] = key
            out[peer, V_AT:Q_AT, :] = value
            out[peer, Q_AT:G_AT, :] = query
            packed = []
            for y in range(4):
                one = gates[h][48 * y : 48 * y + 24]
                two = gates[h][48 * y + 24 : 48 * y + 48]
                if d == 0:
                    packed.append(jnp.where(low_lanes, one, pltpu.roll(two, 64, 1)))
                else:
                    packed.append(jnp.where(low_lanes, pltpu.roll(one, 64, 1), two))
            out[peer, G_AT:S_AT, :] = jnp.concatenate(packed, axis=0).astype(BF16)
            at = 2 * d + h
            four = jnp.concatenate(
                [g_high[at : at + 1], g_low[at : at + 1], b_high[at : at + 1], b_low[at : at + 1],
                 jnp.zeros((4, 256), F32)],
                axis=0,
            )
            out[peer, S_AT:X_ROWS, :] = jnp.concatenate(
                [four[:, :LANES], four[:, LANES:]], axis=0
            ).astype(BF16)


def unit_inverses(lows):
    results = [None] * len(lows)
    largest = max(low.shape[0] for low in lows)
    width = 1
    while width < largest:
        inner = [None] * len(lows)
        for n, low in enumerate(lows):
            size = low.shape[0]
            if width >= size:
                continue
            i, j = iota((size, size), 0), iota((size, size), 1)
            coupled = (i // (2 * width) == j // (2 * width)) & (i // width != j // width)
            coupling = jnp.where(coupled, low, 0.0)
            if width == 1:
                results[n] = jnp.where(i == j, 1.0, 0.0) - coupling
            else:
                inner[n] = (dot(coupling.astype(BF16), results[n].astype(BF16))).astype(BF16)
        if width > 1:
            for n, low in enumerate(lows):
                if inner[n] is not None:
                    results[n] = results[n] - dot(results[n].astype(BF16), inner[n])
        width *= 2
    return results


def token_maps(got, out, reads, offsets, maps, queries):
    backward = lax.rem(lax.axis_index("x"), 2)
    sign = 1 - 2 * backward
    size = CHUNK
    ahead = sign * (iota((size, size), 0) - iota((size, size), 1))
    upto = jnp.where(ahead >= 0, 1.0, 0.0).astype(BF16)
    same = jnp.where(ahead == 0, 1.0, 0.0).astype(BF16)
    low_lanes = iota((8, LANES), 1) < 64

    small = [got[p, S_AT:X_ROWS, :].astype(F32) for p in range(4)]
    first = [s[:8] for s in small]
    second = [s[8:] for s in small]
    turn = lambda v: pltpu.roll(v, 64, 1)
    blocks = [
        first[0],
        jnp.where(low_lanes, second[0], turn(first[1])),
        jnp.where(low_lanes, turn(first[1]), turn(second[1])),
        first[2],
        jnp.where(low_lanes, second[2], turn(first[3])),
        jnp.where(low_lanes, turn(first[3]), turn(second[3])),
    ]
    ctx_lane = iota((8, LANES), 1)
    ctx_small = jnp.zeros((8, LANES), F32)
    for p in range(4):
        here = (ctx_lane >= 8 * p) & (ctx_lane < 8 * p + 8)
        ctx_small = jnp.where(here, pltpu.roll(second[p], (64 + 8 * p) % 128, 1), ctx_small)

    def latent_rows(at, m):
        pieces = {
            0: ((0, 0, 192), (1, 0, 64)),
            1: ((1, 64, 192), (2, 0, 128)),
            2: ((2, 128, 192), (3, 0, 192)),
        }[m]
        return jnp.concatenate([got[p, at + a : at + b, :] for p, a, b in pieces], axis=0)

    def ctx_rows(at):
        return jnp.concatenate(
            [got[p, at + SPAN : at + ROWS, :].astype(F32)[:CTX_OWN] for p in range(4)], axis=0
        ).astype(BF16)

    sets = []
    for m in range(CHUNKS):
        rows = jnp.concatenate([blocks[2 * m], blocks[2 * m + 1]], axis=1).astype(BF16)
        sets.append((latent_rows(K_AT, m), latent_rows(V_AT, m), rows, size, size))
    sets.append((ctx_rows(K_AT), ctx_rows(V_AT), ctx_small.astype(BF16), 32, LANES))

    decays, lows, rights, kept, totals = [], [], [], [], []
    for key, value, rows, n, lanes in sets:
        sums = dot(upto[:n, :lanes], rows, ((1,), (1,)))
        rates = dot(same[:n, :lanes], rows, ((1,), (1,)))
        down = sums[:, 0:1] + sums[:, 1:2]
        beta = rates[:, 2:3] + rates[:, 3:4]
        across = dot(rows, upto[:lanes, :lanes], ((1,), (1,)))
        along = (across[0:1] + across[1:2])[:, :n]
        reach = ahead[:n, :n]
        weights = jnp.where(reach >= 0, jnp.exp(jnp.where(reach >= 0, down - along, 0.0)), 0.0)
        total = jnp.where(backward == 0, down[n - 1 : n], down[0:1])
        key32 = key.astype(F32)
        decayed = jnp.exp(down)
        lows.append(jnp.where(reach > 0, dot(key, key, ((1,), (1,))) * weights * beta, 0.0))
        rights.append(
            jnp.concatenate(
                [(value.astype(F32) * beta).astype(BF16), (key32 * (beta * decayed)).astype(BF16)],
                axis=1,
            )
        )
        kept.append((key32 * jnp.exp(total - down)).astype(BF16))
        totals.append(jnp.exp(total))
        decays.append((decayed, weights))
    inverses = unit_inverses(lows)
    factors = [dot(t.astype(BF16), r).astype(BF16) for t, r in zip(inverses, rights)]

    unit = jnp.where(iota((HEAD, HEAD), 0) == iota((HEAD, HEAD), 1), 1.0, 0.0)
    for m in range(CHUNKS):
        both = dot(kept[m], factors[m], ((0,), (0,)))
        maps[m] = jnp.concatenate([both[:, :HEAD], totals[m] * unit - both[:, HEAD:]], axis=1)
    for m in range(CHUNKS):
        query = latent_rows(Q_AT, m)
        decayed, weights = decays[m]
        pairs = (dot(query, sets[m][0], ((1,), (1,))) * weights).astype(BF16)
        local = dot(pairs, factors[m])
        queries[m] = jnp.concatenate(
            [local[:, :HEAD], query.astype(F32) * decayed - local[:, HEAD:]], axis=1
        )
    so_far = None
    for step in range(CHUNKS):
        m = jnp.where(backward == 0, step, CHUNKS - 1 - step)
        here = queries[m]
        rows = pl.ds(pl.multiple_of(m * CHUNK, CHUNK), CHUNK)
        if step == 0:
            reads[rows, :] = here[:, HEAD:].astype(BF16)
            offsets[rows, :] = here[:, :HEAD]
            so_far = maps[m]
        else:
            moved = dot(here[:, HEAD:].astype(BF16), so_far.astype(BF16))
            reads[rows, :] = moved[:, HEAD:].astype(BF16)
            offsets[rows, :] = here[:, :HEAD] + moved[:, :HEAD]
            mine = maps[m]
            nxt = dot(mine[:, HEAD:].astype(BF16), so_far.astype(BF16))
            so_far = jnp.concatenate([nxt[:, :HEAD] + mine[:, :HEAD], nxt[:, HEAD:]], axis=1)
    whole = so_far.astype(BF16)
    high, low = split_in_two(totals[CHUNKS])
    left = iota((32, LANES), 1) < 64
    tail = jnp.concatenate(
        [kept[CHUNKS], jnp.where(left, high, low).astype(BF16)], axis=1
    )
    for k in range(out.shape[0]):
        out[k, :C_AT, :] = whole
        out[k, C_AT:D_AT, :] = factors[CHUNKS]
        out[k, D_AT:, :] = tail


def read_states(got, reads, offsets, sent, out):
    backward = lax.rem(lax.axis_index("x"), 2)
    place = lax.axis_index("z")
    count = got.shape[0]
    before = jnp.where(backward == 0, place, count - 1 - place)
    ctx_state = jnp.zeros((HEAD, HEAD), F32)
    unit = jnp.where(iota((HEAD, HEAD), 0) == iota((HEAD, HEAD), 1), 1.0, 0.0)
    chain = jnp.concatenate([jnp.zeros((HEAD, HEAD), F32), unit], axis=1)
    for step in range(count):
        k = jnp.where(backward == 0, step, count - 1 - step)
        factor = got[k, C_AT:D_AT, :]
        tail = got[k, D_AT:, :]
        both = tail[0:1, HEAD:].astype(F32)
        kept_share = both[:, 0:1] + both[:, 64:65]
        fresh = factor[:, :HEAD].astype(F32)
        if step > 0:
            fresh = fresh - dot(factor[:, HEAD:], ctx_state.astype(BF16))
        ctx_state = ctx_state * kept_share + dot(tail[:, :HEAD], fresh.astype(BF16), ((0,), (0,)))
        if step < count - 1:
            mine = got[k, :C_AT, :]
            nxt = dot(mine[:, HEAD:], chain.astype(BF16))
            nxt = jnp.concatenate([nxt[:, :HEAD] + mine[:, :HEAD].astype(F32), nxt[:, HEAD:]], axis=1)
            chain = jnp.where(step < before, nxt, chain)
    state = dot(chain[:, HEAD:].astype(BF16), ctx_state.astype(BF16)) + chain[:, :HEAD]
    state = state.astype(BF16)
    for x in range(4):
        rows = slice(SPAN * x, SPAN * x + SPAN)
        o = dot(reads[rows, :], state) + offsets[rows, :]
        gates = sent[x, G_AT:S_AT, :].astype(F32)
        for y in range(4):
            out[4 * x + y] = jnp.concatenate(
                [o[48 * y : 48 * y + 48], gates[24 * y : 24 * y + 24]], axis=0
            ).astype(BF16)


def mix(got, out_gain, gate, w_out, latent, out):
    low_lanes = iota((24, LANES), 1) < 64
    gain = out_gain[...].astype(F32)
    tiles = []
    for y in range(4):
        for h in range(2):
            one = got[8 * h + y].astype(F32)
            two = got[8 * h + 4 + y].astype(F32)
            o = one[:48] + two[:48]
            one, two = one[48:], two[48:]
            gates = jnp.concatenate(
                [
                    jnp.where(low_lanes, one, pltpu.roll(two, 64, 1)),
                    jnp.where(low_lanes, pltpu.roll(one, 64, 1), two),
                ],
                axis=0,
            )
            normed = o * lax.rsqrt(jnp.mean(o * o, axis=-1, keepdims=True) + NORM_EPS)
            tiles.append((normed * gain * gates).astype(BF16))
    gated = jnp.concatenate(tiles, axis=1)
    start = pl.multiple_of(lax.axis_index("tp") * 48, 16)
    own = latent[pl.ds(start, 48), :].astype(F32)
    for n in range(0, D, 512):
        mixed = dot(gated, w_out[:, n : n + 512])
        for c in range(0, 512, LANES):
            j = (n + c) // LANES
            cols = slice(n + c, n + c + LANES)
            out[:, cols] = (own[:, cols] + gate[j : j + 1, :] * mixed[:, c : c + LANES]).astype(BF16)


VM = pl.BlockSpec(memory_space=pltpu.VMEM)


def call(body, name, n_in, outs, scratch=(), mib=16):
    many = isinstance(outs, (list, tuple))
    return pl.pallas_call(
        body,
        out_shape=outs,
        in_specs=[VM] * n_in,
        out_specs=[VM] * len(outs) if many else VM,
        scratch_shapes=list(scratch),
        compiler_params=pltpu.CompilerParams(vmem_limit_bytes=mib << 20),
        name=name,
    )


def shape(dims, dtype=BF16):
    return jax.ShapeDtypeStruct(dims, dtype)


def swap(array, axes):
    return lax.all_to_all(array, axes, 0, 0, tiled=True)


def on_device(
    latent, cond, context, ctx_cond, w_mod, norm_gain, w_query, w_key, w_value, w_outgate,
    w_decay, w_beta, decay_rate, decay_bias, extra_decay, out_gain, w_out,
):
    small = jnp.concatenate([w_decay.reshape(D, 4).T, w_beta.reshape(D, 4).T], axis=0)
    partial = call(
        partial_modulation, "partial_modulation", 3, shape((8, 24, LANES)),
        [pltpu.VMEM((24, LANES), F32)],
    )(cond, ctx_cond[None, :], w_mod)
    summed = call(sum_and_spread, "sum_and_spread", 1, shape((16, 24, LANES)))(swap(partial, "z"))
    parts = swap(summed, ("x", "tp"))
    sent, gate = call(
        project, "project", 12, [shape((4, X_ROWS, LANES)), shape((16, LANES), F32)],
        [pltpu.VMEM((96, LANES), F32), pltpu.VMEM((ROWS, D), BF16)], 24,
    )(
        parts, latent[0], context[0], norm_gain[None, :], w_query, w_key, w_value, w_outgate, small,
        decay_rate.reshape(4, 1), decay_bias.reshape(4, 1), extra_decay.reshape(4, SPAN),
    )
    held = swap(sent, "x")
    maps, reads, offsets = call(
        token_maps, "token_maps", 1,
        [shape((8, Z_ROWS, 256)), shape((ROW_OF_X, HEAD)), shape((ROW_OF_X, HEAD), F32)],
        [pltpu.VMEM((CHUNKS, HEAD, 256), F32), pltpu.VMEM((CHUNKS, CHUNK, 256), F32)],
    )(held)
    reached = swap(maps, "z")
    outs = call(read_states, "read_states", 4, shape((16, 72, LANES)))(
        reached, reads, offsets, held
    )
    own = swap(outs, ("x", "tp"))
    mixed = call(mix, "mix", 5, shape((48, D)))(own, out_gain[None, :], gate, w_out, latent[0])
    return mixed[None]


def solution(mesh):
    torus = Mesh(
        mesh.devices.reshape(8, 4, mesh.shape["tp"], mesh.shape["dp"]), ("z", "x", "tp", "dp")
    )
    sp = ("z", "x")
    return jax.shard_map(
        on_device,
        mesh=torus,
        in_specs=(
            P("dp", sp, None),
            P("dp", sp),
            P("dp", sp, None),
            P(sp),
            P(sp, "tp"),
            P(),
            P(None, "tp"),
            P(None, "tp"),
            P(None, "tp"),
            P(None, "tp"),
            P(None, None, "tp"),
            P(None, None, "tp"),
            P(None, "tp"),
            P(None, "tp"),
            P("dp", None, "tp", sp),
            P(),
            P(),
        ),
        out_specs=P("dp", ("z", "x", "tp"), None),
        check_vma=False,
    )
```

```python
import functools

import jax
import jax.numpy as jnp
from jax import lax
from jax.experimental import pallas as pl
from jax.experimental.pallas import tpu as pltpu
from jax.sharding import Mesh
from jax.sharding import PartitionSpec as P

D = 2048
HEAD = 128
LANES = 128
NORM_EPS = 1e-06
BETA_SCALE = 30.0

SPAN = 192
CTX_OWN = 8
ROWS = 208
CHUNK = 256
CHUNKS = 3
ROW_OF_X = 4 * SPAN

K_AT, V_AT, Q_AT, G_AT, S_AT, X_ROWS = 0, 208, 416, 608, 704, 720
C_AT, D_AT, Z_ROWS = 128, 160, 168

F32 = jnp.float32
BF16 = jnp.bfloat16


def dot(a, b, dims=((1,), (0,))):
    return lax.dot_general(a, b, (dims, ((), ())), preferred_element_type=F32)


def silu(v):
    return v / (1.0 + jnp.exp(-v))


def rounded(v):
    return v.astype(BF16).astype(F32)


def split_in_two(v):
    high = v.astype(BF16)
    return high.astype(F32), v - high.astype(F32)


def iota(shape, dim):
    return lax.broadcasted_iota(jnp.int32, shape, dim)


def fetch(pairs, sems):
    copies = [pltpu.make_async_copy(a, b, sems.at[n]) for n, (a, b) in enumerate(pairs)]
    for copy in copies:
        copy.start()
    return copies


def partial_modulation(cond_in, ctx_cond_in, w_mod_in, out, rows, cond, ctx_cond, w_mod, sems):
    pairs = ((w_mod_in, w_mod), (cond_in, cond), (ctx_cond_in, ctx_cond))
    for copy in fetch(pairs, sems):
        copy.wait()
    first = iota((8, cond.shape[1]), 0) == 0
    values = jnp.where(first, cond[...].astype(F32), ctx_cond[...].astype(F32))
    product = dot(silu(values).astype(BF16), w_mod[...])
    for r in range(2):
        for c in range(12):
            rows[r * 12 + c : r * 12 + c + 1, :] = product[r : r + 1, c * LANES : (c + 1) * LANES]
    value = rows[...].astype(BF16)
    for k in range(out.shape[0]):
        out[k] = value


def sum_and_spread(parts, out):
    total = parts[0].astype(F32)
    for k in range(1, parts.shape[0]):
        total = total + parts[k].astype(F32)
    value = total.astype(BF16)
    for k in range(out.shape[0]):
        out[k] = value


def modulated(values, gain, mods, which):
    scale = lax.rsqrt(jnp.mean(values * values, axis=-1, keepdims=True) + NORM_EPS)

    def row(block):
        at = (block // 12) * 24 + which * 12 + block % 12
        return mods[at : at + 1, :]

    out = []
    for j in range(D // LANES):
        cols = slice(j * LANES, (j + 1) * LANES)
        factor = gain[j : j + 1, :].astype(F32) * (1.0 + row(16 + j))
        out.append((values[:, cols] * scale * factor + row(j)).astype(BF16))
    return out


def project(
    parts, gain_in, decay_in, beta_in, rate_in, bias_in, extra_in, latent_in, context_in,
    w_key_in, w_value_in, w_query_in, w_gate_in, out, gate_out,
    gain, w_decay, w_beta, rate_at, bias_at, extra, latent, context, w_key, w_value, w_query,
    w_gate, sems, mods, rows_in,
):
    copies = fetch(
        (
            (latent_in, latent), (context_in, context), (gain_in, gain), (decay_in, w_decay),
            (beta_in, w_beta), (rate_in, rate_at), (bias_in, bias_at), (extra_in, extra),
            (w_key_in, w_key), (w_value_in, w_value), (w_query_in, w_query), (w_gate_in, w_gate),
        ),
        sems,
    )
    for y in range(4):
        total = parts[y].astype(F32)
        for x in range(1, 4):
            total = total + parts[4 * x + y].astype(F32)
        mods[24 * y : 24 * y + 24, :] = total
    for j in range(16):
        block = 32 + j
        at = (block // 12) * 24 + block % 12
        gate_out[j : j + 1, :] = mods[at : at + 1, :]
    for copy in copies[:8]:
        copy.wait()
    for g in range(0, SPAN, 64):
        for j, tile in enumerate(modulated(latent[0, g : g + 64, :].astype(F32), gain, mods, 0)):
            rows_in[g : g + 64, j * LANES : (j + 1) * LANES] = tile
    ctx_values = jnp.concatenate(
        [context[0].astype(F32), jnp.zeros((ROWS - SPAN - CTX_OWN, D), F32)], axis=0
    )
    for j, tile in enumerate(modulated(ctx_values, gain, mods, 1)):
        rows_in[SPAN:ROWS, j * LANES : (j + 1) * LANES] = tile
    inputs = rows_in[...]

    def heads(values):
        return [values[:, h * HEAD : (h + 1) * HEAD] for h in range(2)]

    def column(at):
        row = iota((4, 1), 0)
        value = jnp.where(row == 0, at[0, 0], at[0, 1])
        return jnp.where(row < 2, value, jnp.where(row == 2, at[1, 0], at[1, 1]))

    w_small = jnp.concatenate(
        [w[d].astype(F32) for w in (w_decay, w_beta) for d in range(2)], axis=0
    ).astype(BF16)
    rate, bias = column(rate_at), column(bias_at)
    small = rounded(dot(w_small, inputs, ((1,), (1,))))
    decay_raw, beta_raw = small[:4], small[4:]
    pre = decay_raw + bias
    soft = jnp.maximum(pre, 0.0) + jnp.log1p(jnp.exp(-jnp.abs(pre)))
    latent_only = jnp.concatenate([extra[0, 0], extra[0, 1]], axis=0)
    added = jnp.concatenate([latent_only, jnp.zeros((4, ROWS - SPAN), F32)], axis=1)
    log_decay = -rate * soft + added
    beta = BETA_SCALE * rate / (1.0 + jnp.exp(-beta_raw))
    pad = jnp.zeros((4, 256 - ROWS), F32)
    g_high, g_low = split_in_two(jnp.concatenate([log_decay, pad], axis=1))
    b_high, b_low = split_in_two(jnp.concatenate([beta, pad], axis=1))

    def unit(v):
        return v * lax.rsqrt(jnp.sum(v * v, axis=-1, keepdims=True) + NORM_EPS)

    copies[8].wait()
    keys = heads(silu(rounded(dot(inputs, w_key[...]))))
    copies[9].wait()
    values = heads(silu(rounded(dot(inputs, w_value[...]))))
    copies[10].wait()
    queries = heads(silu(rounded(dot(inputs[:SPAN], w_query[...]))))
    copies[11].wait()
    gates = heads(silu(rounded(dot(inputs[:SPAN], w_gate[...]))))
    low_lanes = iota((24, LANES), 1) < 64
    for h in range(2):
        key = unit(keys[h]).astype(BF16)
        value = values[h].astype(BF16)
        query = (unit(queries[h]) * HEAD**-0.5).astype(BF16)
        for d in range(2):
            peer = 2 * h + d
            out[peer, K_AT:V_AT, :] = key
            out[peer, V_AT:Q_AT, :] = value
            out[peer, Q_AT:G_AT, :] = query
            packed = []
            for y in range(4):
                one = gates[h][48 * y : 48 * y + 24]
                two = gates[h][48 * y + 24 : 48 * y + 48]
                if d == 0:
                    packed.append(jnp.where(low_lanes, one, pltpu.roll(two, 64, 1)))
                else:
                    packed.append(jnp.where(low_lanes, pltpu.roll(one, 64, 1), two))
            out[peer, G_AT:S_AT, :] = jnp.concatenate(packed, axis=0).astype(BF16)
            at = 2 * d + h
            four = jnp.concatenate(
                [g_high[at : at + 1], g_low[at : at + 1], b_high[at : at + 1], b_low[at : at + 1],
                 jnp.zeros((4, 256), F32)],
                axis=0,
            )
            out[peer, S_AT:X_ROWS, :] = jnp.concatenate(
                [four[:, :LANES], four[:, LANES:]], axis=0
            ).astype(BF16)


def unit_inverses(lows, depths, starts=None):
    width, results = (1, [None] * len(lows)) if starts is None else starts
    while width < max(depths):
        inner = [None] * len(lows)
        for n, low in enumerate(lows):
            if width >= depths[n]:
                continue
            i, j = iota(low.shape, 0), iota(low.shape, 1)
            coupled = (i // (2 * width) == j // (2 * width)) & (i // width != j // width)
            coupling = jnp.where(coupled, low, 0.0)
            if width == 1:
                results[n] = jnp.where(i == j, 1.0, 0.0) - coupling
            else:
                inner[n] = (dot(coupling.astype(BF16), results[n].astype(BF16))).astype(BF16)
        for n in range(len(lows)):
            if inner[n] is not None:
                results[n] = results[n] - dot(results[n].astype(BF16), inner[n])
        width *= 2
    return results


class Order:
    def __init__(self):
        self.backward = lax.rem(lax.axis_index("x"), 2)
        sign = 1 - 2 * self.backward
        self.ahead = sign * (iota((CHUNK, CHUNK), 0) - iota((CHUNK, CHUNK), 1))
        self.upto = jnp.where(self.ahead >= 0, 1.0, 0.0).astype(BF16)
        self.same = jnp.where(self.ahead == 0, 1.0, 0.0).astype(BF16)

    def at(self, step, count):
        return jnp.where(self.backward == 0, step, count - 1 - step)

    def block(self, key, rows):
        n = key.shape[0]
        sums = dot(self.upto[:n, :n], rows, ((1,), (1,)))
        rates = dot(self.same[:n, :n], rows, ((1,), (1,)))
        down = sums[:, 0:1] + sums[:, 1:2]
        beta = rates[:, 2:3] + rates[:, 3:4]
        across = dot(rows, self.upto[:n, :n], ((1,), (1,)))
        along = across[0:1] + across[1:2]
        reach = self.ahead[:n, :n]
        weights = jnp.where(reach >= 0, jnp.exp(jnp.where(reach >= 0, down - along, 0.0)), 0.0)
        total = jnp.where(self.backward == 0, down[n - 1 : n], down[0:1])
        low = jnp.where(reach > 0, dot(key, key, ((1,), (1,))) * weights * beta, 0.0)
        kept = (key.astype(F32) * jnp.exp(total - down)).astype(BF16)
        return low, beta, jnp.exp(down), weights, kept, jnp.exp(total)


def token_maps(got, out, reads, offsets, maps, queries):
    order = Order()
    low_lanes = iota((8, LANES), 1) < 64

    small = [got[p, S_AT:X_ROWS, :].astype(F32) for p in range(4)]
    first = [s[:8] for s in small]
    second = [s[8:] for s in small]
    turn = lambda v: pltpu.roll(v, 64, 1)
    blocks = [
        first[0],
        jnp.where(low_lanes, second[0], turn(first[1])),
        jnp.where(low_lanes, turn(first[1]), turn(second[1])),
        first[2],
        jnp.where(low_lanes, second[2], turn(first[3])),
        jnp.where(low_lanes, turn(first[3]), turn(second[3])),
    ]
    lane = iota((8, LANES), 1)
    ctx_small = jnp.zeros((8, LANES), F32)
    for p in range(4):
        here = (lane >= 8 * p) & (lane < 8 * p + 8)
        ctx_small = jnp.where(here, pltpu.roll(second[p], (64 + 8 * p) % 128, 1), ctx_small)
    ctx_small = ctx_small.astype(BF16)

    def latent_rows(at, m):
        pieces = {
            0: ((0, 0, 192), (1, 0, 64)),
            1: ((1, 64, 192), (2, 0, 128)),
            2: ((2, 128, 192), (3, 0, 192)),
        }[m]
        return jnp.concatenate([got[p, at + a : at + b, :] for p, a, b in pieces], axis=0)

    def ctx_rows(at):
        return jnp.concatenate(
            [got[p, at + SPAN : at + ROWS, :].astype(F32)[:CTX_OWN] for p in range(4)], axis=0
        ).astype(BF16)

    keys = [latent_rows(K_AT, m) for m in range(CHUNKS)]
    rows = [
        jnp.concatenate([blocks[2 * m], blocks[2 * m + 1]], axis=1).astype(BF16)
        for m in range(CHUNKS)
    ]
    ctx_key = ctx_rows(K_AT)
    padded = jnp.concatenate([ctx_key, jnp.zeros((LANES - 32, HEAD), BF16)], axis=0)
    found = [order.block(k, r) for k, r in zip(keys, rows)]
    ctx_low = order.block(padded, ctx_small)[0]
    inverses = unit_inverses([f[0] for f in found] + [ctx_low], [CHUNK] * CHUNKS + [32])
    factors = []
    for m, (_, beta, decayed, _, _, _) in enumerate(found):
        value = (latent_rows(V_AT, m).astype(F32) * beta).astype(BF16)
        key = (keys[m].astype(F32) * (beta * decayed)).astype(BF16)
        factors.append(
            dot(inverses[m].astype(BF16), jnp.concatenate([value, key], axis=1)).astype(BF16)
        )

    unit = jnp.where(iota((HEAD, HEAD), 0) == iota((HEAD, HEAD), 1), 1.0, 0.0)
    for m, (_, _, _, _, kept, total) in enumerate(found):
        both = dot(kept, factors[m], ((0,), (0,)))
        maps[m] = jnp.concatenate([both[:, :HEAD], total * unit - both[:, HEAD:]], axis=1)
    for m, (_, _, decayed, weights, _, _) in enumerate(found):
        query = latent_rows(Q_AT, m)
        pairs = (dot(query, keys[m], ((1,), (1,))) * weights).astype(BF16)
        local = dot(pairs, factors[m])
        queries[m] = jnp.concatenate(
            [local[:, :HEAD], query.astype(F32) * decayed - local[:, HEAD:]], axis=1
        )
    so_far = None
    for step in range(CHUNKS):
        m = order.at(step, CHUNKS)
        here = queries[m]
        at = pl.ds(pl.multiple_of(m * CHUNK, CHUNK), CHUNK)
        if step == 0:
            reads[at, :] = here[:, HEAD:].astype(BF16)
            offsets[at, :] = here[:, :HEAD]
            so_far = maps[m]
        else:
            moved = dot(here[:, HEAD:].astype(BF16), so_far.astype(BF16))
            reads[at, :] = moved[:, HEAD:].astype(BF16)
            offsets[at, :] = here[:, :HEAD] + moved[:, :HEAD]
            mine = maps[m]
            nxt = dot(mine[:, HEAD:].astype(BF16), so_far.astype(BF16))
            so_far = jnp.concatenate([nxt[:, :HEAD] + mine[:, :HEAD], nxt[:, HEAD:]], axis=1)
    whole = so_far.astype(BF16)
    tokens = jnp.concatenate([ctx_key, ctx_rows(V_AT)], axis=1)
    inverse = inverses[CHUNKS]
    packed = inverse[:8]
    for r in range(1, 4):
        packed = jnp.where(
            lane // 32 == r, pltpu.roll(inverse[8 * r : 8 * r + 8], 32 * r, 1), packed
        )
    tail = jnp.concatenate([packed, ctx_small.astype(F32)], axis=1).astype(BF16)
    for k in range(out.shape[0]):
        out[k, :C_AT, :] = whole
        out[k, C_AT:D_AT, :] = tokens
        out[k, D_AT:, :] = tail


def read_states(got, reads, offsets, sent, out):
    order = Order()
    count = got.shape[0]
    before = order.at(lax.axis_index("z"), count)
    unit = jnp.where(iota((HEAD, HEAD), 0) == iota((HEAD, HEAD), 1), 1.0, 0.0)

    key = jnp.concatenate([got[k, C_AT:D_AT, :HEAD] for k in range(count)], axis=0)
    value = jnp.concatenate([got[k, C_AT:D_AT, HEAD:] for k in range(count)], axis=0)
    lane = iota((8, LANES), 1)
    rows = [jnp.zeros((8, LANES), F32)] * 2
    blocks = []
    for k in range(count):
        tail = got[k, D_AT:, :].astype(F32)
        here = lane // 32 == k % 4
        rows[k // 4] = jnp.where(here, pltpu.roll(tail[:, LANES:], 32 * (k % 4), 1), rows[k // 4])
        for r in range(4):
            turned = pltpu.roll(tail[:, :LANES], (32 * (k % 4 - r)) % LANES, 1)
            one = jnp.where(here, turned, 0.0)
            none = jnp.zeros((8, LANES), F32)
            blocks.append(jnp.concatenate([one, none] if k < 4 else [none, one], axis=1))
    start = jnp.concatenate(blocks, axis=0)
    low, beta, _, _, kept, _ = order.block(key, jnp.concatenate(rows, axis=1).astype(BF16))
    inverse = unit_inverses([low], [CHUNK], (32, [start]))[0]
    fresh = dot(inverse.astype(BF16), (value.astype(F32) * beta).astype(BF16))
    ctx_state = dot(kept, fresh.astype(BF16), ((0,), (0,)))

    chain = jnp.concatenate([jnp.zeros((HEAD, HEAD), F32), unit], axis=1)
    for step in range(count - 1):
        mine = got[order.at(step, count), :C_AT, :]
        nxt = dot(mine[:, HEAD:], chain.astype(BF16))
        nxt = jnp.concatenate([nxt[:, :HEAD] + mine[:, :HEAD].astype(F32), nxt[:, HEAD:]], axis=1)
        chain = jnp.where(step < before, nxt, chain)
    state = dot(chain[:, HEAD:].astype(BF16), ctx_state.astype(BF16)) + chain[:, :HEAD]
    state = state.astype(BF16)
    for x in range(4):
        at = slice(SPAN * x, SPAN * x + SPAN)
        o = dot(reads[at, :], state) + offsets[at, :]
        gates = sent[x, G_AT:S_AT, :].astype(F32)
        for y in range(4):
            out[4 * x + y] = jnp.concatenate(
                [o[48 * y : 48 * y + 48], gates[24 * y : 24 * y + 24]], axis=0
            ).astype(BF16)


def mix(got, out_gain, gate, w_out, latent, out):
    low_lanes = iota((24, LANES), 1) < 64
    gain = out_gain[...].astype(F32)
    tiles = []
    for y in range(4):
        for h in range(2):
            one = got[8 * h + y].astype(F32)
            two = got[8 * h + 4 + y].astype(F32)
            o = one[:48] + two[:48]
            one, two = one[48:], two[48:]
            gates = jnp.concatenate(
                [
                    jnp.where(low_lanes, one, pltpu.roll(two, 64, 1)),
                    jnp.where(low_lanes, pltpu.roll(one, 64, 1), two),
                ],
                axis=0,
            )
            normed = o * lax.rsqrt(jnp.mean(o * o, axis=-1, keepdims=True) + NORM_EPS)
            tiles.append((normed * gain * gates).astype(BF16))
    gated = jnp.concatenate(tiles, axis=1)
    start = pl.multiple_of(lax.axis_index("tp") * 48, 16)
    own = latent[pl.ds(start, 48), :].astype(F32)
    for n in range(0, D, 512):
        mixed = dot(gated, w_out[:, n : n + 512])
        for c in range(0, 512, LANES):
            j = (n + c) // LANES
            cols = slice(n + c, n + c + LANES)
            out[:, cols] = (own[:, cols] + gate[j : j + 1, :] * mixed[:, c : c + LANES]).astype(BF16)


VM = pl.BlockSpec(memory_space=pltpu.VMEM)


HBM = pl.BlockSpec(memory_space=pltpu.HBM)


def call(body, name, n_in, outs, scratch=(), mib=16, n_hbm=0):
    many = isinstance(outs, (list, tuple))
    return pl.pallas_call(
        body,
        out_shape=outs,
        in_specs=[VM] * n_in + [HBM] * n_hbm,
        out_specs=[VM] * len(outs) if many else VM,
        scratch_shapes=list(scratch),
        compiler_params=pltpu.CompilerParams(vmem_limit_bytes=mib << 20),
        name=name,
    )


def shape(dims, dtype=BF16):
    return jax.ShapeDtypeStruct(dims, dtype)


def swap(array, axes):
    return lax.all_to_all(array, axes, 0, 0, tiled=True)


def on_device(
    latent, cond, context, ctx_cond, w_mod, norm_gain, w_query, w_key, w_value, w_outgate,
    w_decay, w_beta, decay_rate, decay_bias, extra_decay, out_gain, w_out,
):
    partial = call(
        partial_modulation, "partial_modulation", 0, shape((8, 24, LANES)),
        [
            pltpu.VMEM((24, LANES), F32), pltpu.VMEM(cond.shape, BF16),
            pltpu.VMEM(cond.shape, BF16), pltpu.VMEM(w_mod.shape, BF16),
            pltpu.SemaphoreType.DMA((3,)),
        ],
        58, 3,
    )(cond, ctx_cond[None, :], w_mod)
    summed = call(sum_and_spread, "sum_and_spread", 1, shape((16, 24, LANES)))(swap(partial, "z"))
    parts = swap(summed, ("x", "tp"))
    by_row = lambda w: w.transpose(1, 2, 0)
    fetched = (
        norm_gain.reshape(16, LANES), by_row(w_decay), by_row(w_beta), decay_rate, decay_bias,
        extra_decay, latent, context, w_key, w_value, w_query, w_outgate,
    )
    space = lambda n: pltpu.SMEM if n in (3, 4) else pltpu.VMEM
    sent, gate = call(
        project, "project", 1, [shape((4, X_ROWS, LANES)), shape((16, LANES), F32)],
        [space(n)(a.shape, a.dtype) for n, a in enumerate(fetched)]
        + [
            pltpu.SemaphoreType.DMA((len(fetched),)), pltpu.VMEM((96, LANES), F32),
            pltpu.VMEM((ROWS, D), BF16),
        ],
        58, len(fetched),
    )(parts, *fetched)
    held = swap(sent, "x")
    maps, reads, offsets = call(
        token_maps, "token_maps", 1,
        [shape((8, Z_ROWS, 256)), shape((ROW_OF_X, HEAD)), shape((ROW_OF_X, HEAD), F32)],
        [pltpu.VMEM((CHUNKS, HEAD, 256), F32), pltpu.VMEM((CHUNKS, CHUNK, 256), F32)],
    )(held)
    reached = swap(maps, "z")
    outs = call(read_states, "read_states", 4, shape((16, 72, LANES)))(
        reached, reads, offsets, held
    )
    own = swap(outs, ("x", "tp"))
    mixed = call(mix, "mix", 5, shape((48, D)))(own, out_gain[None, :], gate, w_out, latent[0])
    return mixed[None]


def solution(mesh):
    torus = Mesh(
        mesh.devices.reshape(8, 4, mesh.shape["tp"], mesh.shape["dp"]), ("z", "x", "tp", "dp")
    )
    sp = ("z", "x")
    return jax.shard_map(
        on_device,
        mesh=torus,
        in_specs=(
            P("dp", sp, None),
            P("dp", sp),
            P("dp", sp, None),
            P(sp),
            P(sp, "tp"),
            P(),
            P(None, "tp"),
            P(None, "tp"),
            P(None, "tp"),
            P(None, "tp"),
            P(None, None, "tp"),
            P(None, None, "tp"),
            P(None, "tp"),
            P(None, "tp"),
            P("dp", None, "tp", sp),
            P(),
            P(),
        ),
        out_specs=P("dp", ("z", "x", "tp"), None),
        check_vma=False,
    )
```

```python
import functools

import jax
import jax.numpy as jnp
from jax import lax
from jax.experimental import pallas as pl
from jax.experimental.pallas import tpu as pltpu
from jax.sharding import Mesh
from jax.sharding import PartitionSpec as P

D = 2048
HEAD = 128
LANES = 128
NORM_EPS = 1e-06
BETA_SCALE = 30.0

SPAN = 192
CTX_OWN = 8
ROWS = 208
CHUNK = 256
CHUNKS = 3
ROW_OF_X = 4 * SPAN

K_AT, V_AT, Q_AT, G_AT, S_AT, X_ROWS = 0, 208, 416, 608, 704, 720
C_AT, D_AT, Z_ROWS = 128, 160, 168

F32 = jnp.float32
BF16 = jnp.bfloat16


def dot(a, b, dims=((1,), (0,))):
    return lax.dot_general(a, b, (dims, ((), ())), preferred_element_type=F32)


def silu(v):
    return v / (1.0 + jnp.exp(-v))


def rounded(v):
    return v.astype(BF16).astype(F32)


def split_in_two(v):
    high = v.astype(BF16)
    return high.astype(F32), v - high.astype(F32)


def iota(shape, dim):
    return lax.broadcasted_iota(jnp.int32, shape, dim)


def fetch(pairs, sems):
    copies = [pltpu.make_async_copy(a, b, sems.at[n]) for n, (a, b) in enumerate(pairs)]
    for copy in copies:
        copy.start()
    return copies


def partial_modulation(cond_in, ctx_cond_in, w_mod_in, out, rows, cond, ctx_cond, w_mod, sems):
    pairs = ((w_mod_in, w_mod), (cond_in, cond), (ctx_cond_in, ctx_cond))
    for copy in fetch(pairs, sems):
        copy.wait()
    first = iota((8, cond.shape[1]), 0) == 0
    values = jnp.where(first, cond[...].astype(F32), ctx_cond[...].astype(F32))
    product = dot(silu(values).astype(BF16), w_mod[...])
    for r in range(2):
        for c in range(12):
            rows[r * 12 + c : r * 12 + c + 1, :] = product[r : r + 1, c * LANES : (c + 1) * LANES]
    value = rows[...].astype(BF16)
    for k in range(out.shape[0]):
        out[k] = value


def sum_and_spread(parts, out):
    total = parts[0].astype(F32)
    for k in range(1, parts.shape[0]):
        total = total + parts[k].astype(F32)
    value = total.astype(BF16)
    for k in range(out.shape[0]):
        out[k] = value


def prepare(
    gain_in, decay_in, beta_in, rate_in, bias_in, extra_in, latent_in, context_in,
    w_key_in, w_value_in, w_key, w_value, latent, context, factors, gain, w_small, consts,
    w_decay, w_beta, rate, bias, extra, sems,
):
    copies = fetch(
        (
            (latent_in, latent), (context_in, context), (gain_in, gain), (decay_in, w_decay),
            (beta_in, w_beta), (rate_in, rate), (bias_in, bias), (extra_in, extra),
            (w_key_in, w_key), (w_value_in, w_value),
        ),
        sems,
    )
    for copy in copies[:8]:
        copy.wait()

    def factor(values):
        values = values.astype(F32)
        mean = jnp.mean(values * values, axis=-1, keepdims=True)
        return jnp.broadcast_to(lax.rsqrt(mean + NORM_EPS), (values.shape[0], LANES))

    for g in range(0, SPAN, 64):
        factors[g : g + 64, :] = factor(latent[0, g : g + 64, :])
    factors[SPAN : SPAN + CTX_OWN, :] = factor(context[0])
    factors[SPAN + CTX_OWN :, :] = jnp.zeros((ROWS - SPAN - CTX_OWN, LANES), F32)
    w_small[...] = jnp.concatenate(
        [w[d].astype(F32) for w in (w_decay, w_beta) for d in range(2)], axis=0
    ).astype(BF16)

    def spread(at):
        row = iota((4, 256), 0)
        value = jnp.where(row == 0, at[0, 0], at[0, 1])
        return jnp.where(row < 2, value, jnp.where(row == 2, at[1, 0], at[1, 1]))

    latent_only = jnp.concatenate([extra[0, 0], extra[0, 1]], axis=0)
    added = jnp.concatenate([latent_only, jnp.zeros((4, 256 - SPAN), F32)], axis=1)
    consts[...] = jnp.concatenate(
        [added, spread(rate), spread(bias), jnp.zeros((4, 256), F32)], axis=0
    )
    for copy in copies[8:]:
        copy.wait()


def project(
    parts, w_key, w_value, latent, context, factors, gain, w_small, consts, w_query_in, w_gate_in,
    out, gate_out, mods, rows_in, w_query, w_gate, sems,
):
    copies = fetch(((w_query_in, w_query), (w_gate_in, w_gate)), sems)
    for y in range(4):
        total = parts[y].astype(F32)
        for x in range(1, 4):
            total = total + parts[4 * x + y].astype(F32)
        mods[24 * y : 24 * y + 24, :] = total

    def row(which, block):
        at = (block // 12) * 24 + which * 12 + block % 12
        return mods[at : at + 1, :]

    for j in range(16):
        gate_out[j : j + 1, :] = row(0, 32 + j)
    none = jnp.zeros((ROWS - SPAN - CTX_OWN, LANES), F32)
    for which, rows in ((0, slice(0, SPAN)), (1, slice(SPAN, ROWS))):
        for j in range(16):
            cols = slice(j * LANES, (j + 1) * LANES)
            if which == 0:
                values = latent[0, :, cols].astype(F32)
            else:
                values = jnp.concatenate([context[0, :, cols].astype(F32), none], axis=0)
            scale = gain[j : j + 1, :].astype(F32) * (1.0 + row(which, 16 + j))
            tile = values * factors[rows, :] * scale + row(which, j)
            rows_in[rows, cols] = tile.astype(BF16)
    inputs = rows_in[...]

    def heads(values):
        return [values[:, h * HEAD : (h + 1) * HEAD] for h in range(2)]

    added, rate, bias = (consts[n : n + 4, :ROWS] for n in (0, 4, 8))
    small = rounded(dot(w_small[...], inputs, ((1,), (1,))))
    decay_raw, beta_raw = small[:4], small[4:]
    pre = decay_raw + bias
    soft = jnp.maximum(pre, 0.0) + jnp.log1p(jnp.exp(-jnp.abs(pre)))
    log_decay = -rate * soft + added
    beta = BETA_SCALE * rate / (1.0 + jnp.exp(-beta_raw))
    pad = jnp.zeros((4, 256 - ROWS), F32)
    g_high, g_low = split_in_two(jnp.concatenate([log_decay, pad], axis=1))
    b_high, b_low = split_in_two(jnp.concatenate([beta, pad], axis=1))

    def unit(v):
        return v * lax.rsqrt(jnp.sum(v * v, axis=-1, keepdims=True) + NORM_EPS)

    keys = heads(silu(rounded(dot(inputs, w_key[...]))))
    values = heads(silu(rounded(dot(inputs, w_value[...]))))
    copies[0].wait()
    queries = heads(silu(rounded(dot(inputs[:SPAN], w_query[...]))))
    copies[1].wait()
    gates = heads(silu(rounded(dot(inputs[:SPAN], w_gate[...]))))
    low_lanes = iota((24, LANES), 1) < 64
    for h in range(2):
        key = unit(keys[h]).astype(BF16)
        value = values[h].astype(BF16)
        query = (unit(queries[h]) * HEAD**-0.5).astype(BF16)
        for d in range(2):
            peer = 2 * h + d
            out[peer, K_AT:V_AT, :] = key
            out[peer, V_AT:Q_AT, :] = value
            out[peer, Q_AT:G_AT, :] = query
            packed = []
            for y in range(4):
                one = gates[h][48 * y : 48 * y + 24]
                two = gates[h][48 * y + 24 : 48 * y + 48]
                if d == 0:
                    packed.append(jnp.where(low_lanes, one, pltpu.roll(two, 64, 1)))
                else:
                    packed.append(jnp.where(low_lanes, pltpu.roll(one, 64, 1), two))
            out[peer, G_AT:S_AT, :] = jnp.concatenate(packed, axis=0).astype(BF16)
            at = 2 * d + h
            four = jnp.concatenate(
                [g_high[at : at + 1], g_low[at : at + 1], b_high[at : at + 1], b_low[at : at + 1],
                 jnp.zeros((4, 256), F32)],
                axis=0,
            )
            out[peer, S_AT:X_ROWS, :] = jnp.concatenate(
                [four[:, :LANES], four[:, LANES:]], axis=0
            ).astype(BF16)


def unit_inverses(lows, depths, starts=None):
    width, results = (1, [None] * len(lows)) if starts is None else starts
    while width < max(depths):
        inner = [None] * len(lows)
        for n, low in enumerate(lows):
            if width >= depths[n]:
                continue
            i, j = iota(low.shape, 0), iota(low.shape, 1)
            coupled = (i // (2 * width) == j // (2 * width)) & (i // width != j // width)
            coupling = jnp.where(coupled, low, 0.0)
            if width == 1:
                results[n] = jnp.where(i == j, 1.0, 0.0) - coupling
            else:
                inner[n] = (dot(coupling.astype(BF16), results[n].astype(BF16))).astype(BF16)
        for n in range(len(lows)):
            if inner[n] is not None:
                results[n] = results[n] - dot(results[n].astype(BF16), inner[n])
        width *= 2
    return results


class Order:
    def __init__(self):
        self.backward = lax.rem(lax.axis_index("x"), 2)
        sign = 1 - 2 * self.backward
        self.ahead = sign * (iota((CHUNK, CHUNK), 0) - iota((CHUNK, CHUNK), 1))
        self.upto = jnp.where(self.ahead >= 0, 1.0, 0.0).astype(BF16)
        self.same = jnp.where(self.ahead == 0, 1.0, 0.0).astype(BF16)

    def at(self, step, count):
        return jnp.where(self.backward == 0, step, count - 1 - step)

    def decays(self, rows):
        n = rows.shape[1]
        sums = dot(self.upto[:n, :n], rows, ((1,), (1,)))
        down = sums[:, 0:1] + sums[:, 1:2]
        across = dot(rows, self.upto[:n, :n], ((1,), (1,)))
        along = across[0:1] + across[1:2]
        reach = self.ahead[:n, :n]
        weights = jnp.where(reach >= 0, jnp.exp(jnp.where(reach >= 0, down - along, 0.0)), 0.0)
        return down, weights

    def block(self, key, rows):
        n = key.shape[0]
        down, weights = self.decays(rows)
        rates = dot(self.same[:n, :n], rows, ((1,), (1,)))
        beta = rates[:, 2:3] + rates[:, 3:4]
        total = jnp.where(self.backward == 0, down[n - 1 : n], down[0:1])
        reach = self.ahead[:n, :n]
        low = jnp.where(reach > 0, dot(key, key, ((1,), (1,))) * weights * beta, 0.0)
        kept = (key.astype(F32) * jnp.exp(total - down)).astype(BF16)
        return low, beta, jnp.exp(down), kept, jnp.exp(total)


def small_rows(got):
    low_lanes = iota((8, LANES), 1) < 64
    small = [got[p, S_AT:X_ROWS, :].astype(F32) for p in range(4)]
    first = [s[:8] for s in small]
    second = [s[8:] for s in small]
    turn = lambda v: pltpu.roll(v, 64, 1)
    blocks = [
        first[0],
        jnp.where(low_lanes, second[0], turn(first[1])),
        jnp.where(low_lanes, turn(first[1]), turn(second[1])),
        first[2],
        jnp.where(low_lanes, second[2], turn(first[3])),
        jnp.where(low_lanes, turn(first[3]), turn(second[3])),
    ]
    lane = iota((8, LANES), 1)
    ctx_small = jnp.zeros((8, LANES), F32)
    for p in range(4):
        here = (lane >= 8 * p) & (lane < 8 * p + 8)
        ctx_small = jnp.where(here, pltpu.roll(second[p], (64 + 8 * p) % 128, 1), ctx_small)
    rows = [
        jnp.concatenate([blocks[2 * m], blocks[2 * m + 1]], axis=1).astype(BF16)
        for m in range(CHUNKS)
    ]
    return rows, ctx_small.astype(BF16)


def latent_rows(got, at, m):
    pieces = {
        0: ((0, 0, 192), (1, 0, 64)),
        1: ((1, 64, 192), (2, 0, 128)),
        2: ((2, 128, 192), (3, 0, 192)),
    }[m]
    return jnp.concatenate([got[p, at + a : at + b, :] for p, a, b in pieces], axis=0)


def add_block(mine, so_far):
    nxt = dot(mine[:, HEAD:].astype(BF16), so_far.astype(BF16))
    return jnp.concatenate([nxt[:, :HEAD] + mine[:, :HEAD].astype(F32), nxt[:, HEAD:]], axis=1)


def token_maps(got, out, reads, offsets, factors, maps, queries):
    order = Order()

    def ctx_rows(at):
        return jnp.concatenate(
            [got[p, at + SPAN : at + ROWS, :].astype(F32)[:CTX_OWN] for p in range(4)], axis=0
        ).astype(BF16)

    rows, ctx_small = small_rows(got)
    keys = [latent_rows(got, K_AT, m) for m in range(CHUNKS)]
    ctx_key = ctx_rows(K_AT)
    padded = jnp.concatenate([ctx_key, jnp.zeros((LANES - 32, HEAD), BF16)], axis=0)
    found = [order.block(k, r) for k, r in zip(keys, rows)]
    ctx_low = order.block(padded, ctx_small)[0]
    inverses = unit_inverses([f[0] for f in found] + [ctx_low], [CHUNK] * CHUNKS + [32])
    for m, (_, beta, decayed, _, _) in enumerate(found):
        value = (latent_rows(got, V_AT, m).astype(F32) * beta).astype(BF16)
        key = (keys[m].astype(F32) * (beta * decayed)).astype(BF16)
        right = jnp.concatenate([value, key], axis=1)
        factors[m] = dot(inverses[m].astype(BF16), right).astype(BF16)
    unit = jnp.where(iota((HEAD, HEAD), 0) == iota((HEAD, HEAD), 1), 1.0, 0.0)
    for m, (_, _, _, kept, total) in enumerate(found):
        both = dot(kept, factors[m], ((0,), (0,)))
        maps[m] = jnp.concatenate([both[:, :HEAD], total * unit - both[:, HEAD:]], axis=1)
    so_far = maps[order.at(0, CHUNKS)]
    for step in range(1, CHUNKS):
        so_far = add_block(maps[order.at(step, CHUNKS)], so_far)
    whole = so_far.astype(BF16)
    tokens = jnp.concatenate([ctx_key, ctx_rows(V_AT)], axis=1)
    token_reads(got, order, rows, factors, maps, reads, offsets, queries)
    inverse = inverses[CHUNKS]
    lane = iota((8, LANES), 1)
    packed = inverse[:8]
    for r in range(1, 4):
        packed = jnp.where(
            lane // 32 == r, pltpu.roll(inverse[8 * r : 8 * r + 8], 32 * r, 1), packed
        )
    tail = jnp.concatenate([packed, ctx_small.astype(F32)], axis=1).astype(BF16)
    for k in range(out.shape[0]):
        out[k, :C_AT, :] = whole
        out[k, C_AT:D_AT, :] = tokens
        out[k, D_AT:, :] = tail


def token_reads(got, order, rows, factors, maps, reads, offsets, queries):
    for m in range(CHUNKS):
        down, weights = order.decays(rows[m])
        query = latent_rows(got, Q_AT, m)
        pairs = (dot(query, latent_rows(got, K_AT, m), ((1,), (1,))) * weights).astype(BF16)
        local = dot(pairs, factors[m])
        queries[m] = jnp.concatenate(
            [local[:, :HEAD], query.astype(F32) * jnp.exp(down) - local[:, HEAD:]], axis=1
        )
    so_far = None
    for step in range(CHUNKS):
        m = order.at(step, CHUNKS)
        here = queries[m]
        at = pl.ds(pl.multiple_of(m * CHUNK, CHUNK), CHUNK)
        if step == 0:
            reads[at, :] = here[:, HEAD:].astype(BF16)
            offsets[at, :] = here[:, :HEAD]
            so_far = maps[m]
        else:
            moved = dot(here[:, HEAD:].astype(BF16), so_far.astype(BF16))
            reads[at, :] = moved[:, HEAD:].astype(BF16)
            offsets[at, :] = here[:, :HEAD] + moved[:, :HEAD]
            if step < CHUNKS - 1:
                so_far = add_block(maps[m], so_far)


def read_states(got, reads, offsets, sent, out):
    order = Order()
    count = got.shape[0]
    before = order.at(lax.axis_index("z"), count)
    unit = jnp.where(iota((HEAD, HEAD), 0) == iota((HEAD, HEAD), 1), 1.0, 0.0)

    key = jnp.concatenate([got[k, C_AT:D_AT, :HEAD] for k in range(count)], axis=0)
    value = jnp.concatenate([got[k, C_AT:D_AT, HEAD:] for k in range(count)], axis=0)
    lane = iota((8, LANES), 1)
    rows = [jnp.zeros((8, LANES), F32)] * 2
    blocks = []
    for k in range(count):
        tail = got[k, D_AT:, :].astype(F32)
        here = lane // 32 == k % 4
        rows[k // 4] = jnp.where(here, pltpu.roll(tail[:, LANES:], 32 * (k % 4), 1), rows[k // 4])
        for r in range(4):
            turned = pltpu.roll(tail[:, :LANES], (32 * (k % 4 - r)) % LANES, 1)
            one = jnp.where(here, turned, 0.0)
            none = jnp.zeros((8, LANES), F32)
            blocks.append(jnp.concatenate([one, none] if k < 4 else [none, one], axis=1))
    start = jnp.concatenate(blocks, axis=0)
    low, beta, _, kept, _ = order.block(key, jnp.concatenate(rows, axis=1).astype(BF16))
    inverse = unit_inverses([low], [CHUNK], (32, [start]))[0]
    fresh = dot(inverse.astype(BF16), (value.astype(F32) * beta).astype(BF16))
    ctx_state = dot(kept, fresh.astype(BF16), ((0,), (0,)))

    chain = jnp.concatenate([jnp.zeros((HEAD, HEAD), F32), unit], axis=1)
    for step in range(count - 1):
        nxt = add_block(got[order.at(step, count), :C_AT, :], chain)
        chain = jnp.where(step < before, nxt, chain)
    state = dot(chain[:, HEAD:].astype(BF16), ctx_state.astype(BF16)) + chain[:, :HEAD]
    state = state.astype(BF16)
    for x in range(4):
        at = slice(SPAN * x, SPAN * x + SPAN)
        o = dot(reads[at, :], state) + offsets[at, :]
        gates = sent[x, G_AT:S_AT, :].astype(F32)
        for y in range(4):
            out[4 * x + y] = jnp.concatenate(
                [o[48 * y : 48 * y + 48], gates[24 * y : 24 * y + 24]], axis=0
            ).astype(BF16)


def mix(got, out_gain, gate, w_out, latent, out):
    low_lanes = iota((24, LANES), 1) < 64
    gain = out_gain[...].astype(F32)
    tiles = []
    for y in range(4):
        for h in range(2):
            one = got[8 * h + y].astype(F32)
            two = got[8 * h + 4 + y].astype(F32)
            o = one[:48] + two[:48]
            one, two = one[48:], two[48:]
            gates = jnp.concatenate(
                [
                    jnp.where(low_lanes, one, pltpu.roll(two, 64, 1)),
                    jnp.where(low_lanes, pltpu.roll(one, 64, 1), two),
                ],
                axis=0,
            )
            normed = o * lax.rsqrt(jnp.mean(o * o, axis=-1, keepdims=True) + NORM_EPS)
            tiles.append((normed * gain * gates).astype(BF16))
    gated = jnp.concatenate(tiles, axis=1)
    start = pl.multiple_of(lax.axis_index("tp") * 48, 16)
    own = latent[pl.ds(start, 48), :].astype(F32)
    for n in range(0, D, 512):
        mixed = dot(gated, w_out[:, n : n + 512])
        for c in range(0, 512, LANES):
            j = (n + c) // LANES
            cols = slice(n + c, n + c + LANES)
            out[:, cols] = (own[:, cols] + gate[j : j + 1, :] * mixed[:, c : c + LANES]).astype(BF16)


VM = pl.BlockSpec(memory_space=pltpu.VMEM)


HBM = pl.BlockSpec(memory_space=pltpu.HBM)


def call(body, name, n_in, outs, scratch=(), mib=16, n_hbm=0):
    many = isinstance(outs, (list, tuple))
    return pl.pallas_call(
        body,
        out_shape=outs,
        in_specs=[VM] * n_in + [HBM] * n_hbm,
        out_specs=[VM] * len(outs) if many else VM,
        scratch_shapes=list(scratch),
        compiler_params=pltpu.CompilerParams(vmem_limit_bytes=mib << 20),
        name=name,
    )


def shape(dims, dtype=BF16):
    return jax.ShapeDtypeStruct(dims, dtype)


def in_hbm(array):
    return pltpu.with_memory_space_constraint(array, pltpu.HBM)


def swap(array, axes):
    return lax.all_to_all(array, axes, 0, 0, tiled=True)


def on_device(
    latent, cond, context, ctx_cond, w_mod, norm_gain, w_query, w_key, w_value, w_outgate,
    w_decay, w_beta, decay_rate, decay_bias, extra_decay, out_gain, w_out,
):
    by_row = lambda w: w.transpose(1, 2, 0)
    fetched = (
        norm_gain.reshape(16, LANES), by_row(w_decay), by_row(w_beta), decay_rate, decay_bias,
        extra_decay, latent, context, w_key, w_value,
    )
    space = lambda n: pltpu.SMEM if n in (3, 4) else pltpu.VMEM
    prepared = call(
        prepare, "prepare", 0,
        [shape(w.shape) for w in fetched[8:]]
        + [
            shape(latent.shape), shape(context.shape), shape((ROWS, LANES), F32),
            shape((16, LANES)), shape((8, D)), shape((16, 256), F32),
        ],
        [space(n)(a.shape, a.dtype) for n, a in enumerate(fetched) if 1 <= n <= 5]
        + [pltpu.SemaphoreType.DMA((len(fetched),))],
        16, len(fetched),
    )(*(in_hbm(a) for a in fetched))
    partial = call(
        partial_modulation, "partial_modulation", 0, shape((8, 24, LANES)),
        [
            pltpu.VMEM((24, LANES), F32), pltpu.VMEM(cond.shape, BF16),
            pltpu.VMEM(cond.shape, BF16), pltpu.VMEM(w_mod.shape, BF16),
            pltpu.SemaphoreType.DMA((3,)),
        ],
        16, 3,
    )(in_hbm(cond), in_hbm(ctx_cond[None, :]), in_hbm(w_mod))
    summed = call(sum_and_spread, "sum_and_spread", 1, shape((16, 24, LANES)))(swap(partial, "z"))
    parts = swap(summed, ("x", "tp"))
    sent, gate = call(
        project, "project", 1 + len(prepared), [shape((4, X_ROWS, LANES)), shape((16, LANES), F32)],
        [pltpu.VMEM((96, LANES), F32), pltpu.VMEM((ROWS, D), BF16)]
        + [pltpu.VMEM(w_query.shape, BF16)] * 2 + [pltpu.SemaphoreType.DMA((2,))],
        24, 2,
    )(parts, *prepared, in_hbm(w_query), in_hbm(w_outgate))
    held = swap(sent, "x")
    maps, reads, offsets = call(
        token_maps, "token_maps", 1,
        [shape((8, Z_ROWS, 256)), shape((ROW_OF_X, HEAD)), shape((ROW_OF_X, HEAD), F32)],
        [
            pltpu.VMEM((CHUNKS, CHUNK, 256), BF16), pltpu.VMEM((CHUNKS, HEAD, 256), F32),
            pltpu.VMEM((CHUNKS, CHUNK, 256), F32),
        ],
    )(held)
    reached = swap(maps, "z")
    outs = call(read_states, "read_states", 4, shape((16, 72, LANES)))(
        reached, reads, offsets, held
    )
    gathered = swap(outs, ("x", "tp"))
    mixed = call(mix, "mix", 5, shape((48, D)))(
        gathered, out_gain[None, :], gate, w_out, latent[0]
    )
    return mixed[None]


def solution(mesh):
    torus = Mesh(
        mesh.devices.reshape(8, 4, mesh.shape["tp"], mesh.shape["dp"]), ("z", "x", "tp", "dp")
    )
    sp = ("z", "x")
    return jax.shard_map(
        on_device,
        mesh=torus,
        in_specs=(
            P("dp", sp, None),
            P("dp", sp),
            P("dp", sp, None),
            P(sp),
            P(sp, "tp"),
            P(),
            P(None, "tp"),
            P(None, "tp"),
            P(None, "tp"),
            P(None, "tp"),
            P(None, None, "tp"),
            P(None, None, "tp"),
            P(None, "tp"),
            P(None, "tp"),
            P("dp", None, "tp", sp),
            P(),
            P(),
        ),
        out_specs=P("dp", ("z", "x", "tp"), None),
        check_vma=False,
    )
```

```python
import functools

import jax
import jax.numpy as jnp
from jax import lax
from jax.experimental import pallas as pl
from jax.experimental.pallas import tpu as pltpu
from jax.sharding import Mesh
from jax.sharding import PartitionSpec as P

D = 2048
HEAD = 128
LANES = 128
NORM_EPS = 1e-06
BETA_SCALE = 30.0

SPAN = 192
CTX_OWN = 8
ROWS = 208
CHUNK = 256
CHUNKS = 3
ROW_OF_X = 4 * SPAN

K_AT, V_AT, Q_AT, S_AT, X_ROWS = 0, 208, 416, 608, 624

F32 = jnp.float32
BF16 = jnp.bfloat16


def dot(a, b, dims=((1,), (0,))):
    return lax.dot_general(a, b, (dims, ((), ())), preferred_element_type=F32)


def silu(v):
    return v / (1.0 + jnp.exp(-v))


def rounded(v):
    return v.astype(BF16).astype(F32)


def split_in_two(v):
    high = v.astype(BF16)
    return high.astype(F32), v - high.astype(F32)


def iota(shape, dim):
    return lax.broadcasted_iota(jnp.int32, shape, dim)


def fetch(pairs, sems):
    copies = [pltpu.make_async_copy(a, b, sems.at[n]) for n, (a, b) in enumerate(pairs)]
    for copy in copies:
        copy.start()
    return copies


def partial_modulation(cond_in, ctx_cond_in, w_mod_in, out, rows, cond, ctx_cond, w_mod, sems):
    pairs = ((w_mod_in, w_mod), (cond_in, cond), (ctx_cond_in, ctx_cond))
    for copy in fetch(pairs, sems):
        copy.wait()
    first = iota((8, cond.shape[1]), 0) == 0
    values = jnp.where(first, cond[...].astype(F32), ctx_cond[...].astype(F32))
    product = dot(silu(values).astype(BF16), w_mod[...])
    for r in range(2):
        for c in range(12):
            rows[r * 12 + c : r * 12 + c + 1, :] = product[r : r + 1, c * LANES : (c + 1) * LANES]
    value = rows[...].astype(BF16)
    for k in range(out.shape[0]):
        out[k] = value


def sum_and_spread(parts, out):
    total = parts[0].astype(F32)
    for k in range(1, parts.shape[0]):
        total = total + parts[k].astype(F32)
    value = total.astype(BF16)
    for k in range(out.shape[0]):
        out[k] = value


def prepare(
    gain_in, decay_in, beta_in, rate_in, bias_in, extra_in, latent_in, context_in,
    w_key_in, w_value_in, w_key, w_value, latent, context, factors, gain, w_small, consts,
    w_decay, w_beta, rate, bias, extra, sems,
):
    copies = fetch(
        (
            (latent_in, latent), (context_in, context), (gain_in, gain), (decay_in, w_decay),
            (beta_in, w_beta), (rate_in, rate), (bias_in, bias), (extra_in, extra),
            (w_key_in, w_key), (w_value_in, w_value),
        ),
        sems,
    )
    for copy in copies[:8]:
        copy.wait()

    def factor(values):
        values = values.astype(F32)
        mean = jnp.mean(values * values, axis=-1, keepdims=True)
        return jnp.broadcast_to(lax.rsqrt(mean + NORM_EPS), (values.shape[0], LANES))

    for g in range(0, SPAN, 64):
        factors[g : g + 64, :] = factor(latent[0, g : g + 64, :])
    factors[SPAN : SPAN + CTX_OWN, :] = factor(context[0])
    factors[SPAN + CTX_OWN :, :] = jnp.zeros((ROWS - SPAN - CTX_OWN, LANES), F32)
    w_small[...] = jnp.concatenate(
        [w[d].astype(F32) for w in (w_decay, w_beta) for d in range(2)], axis=0
    ).astype(BF16)

    def spread(at):
        row = iota((4, 256), 0)
        value = jnp.where(row == 0, at[0, 0], at[0, 1])
        return jnp.where(row < 2, value, jnp.where(row == 2, at[1, 0], at[1, 1]))

    latent_only = jnp.concatenate([extra[0, 0], extra[0, 1]], axis=0)
    added = jnp.concatenate([latent_only, jnp.zeros((4, 256 - SPAN), F32)], axis=1)
    consts[...] = jnp.concatenate(
        [added, spread(rate), spread(bias), jnp.zeros((4, 256), F32)], axis=0
    )
    for copy in copies[8:]:
        copy.wait()


def project(
    parts, w_key, w_value, latent, context, factors, gain, w_small, consts, w_query_in, w_gate_in,
    out, gate_out, mods, rows_in, w_query, w_gate, sems,
):
    copies = fetch(((w_query_in, w_query), (w_gate_in, w_gate)), sems)
    for y in range(4):
        total = parts[y].astype(F32)
        for x in range(1, 4):
            total = total + parts[4 * x + y].astype(F32)
        mods[24 * y : 24 * y + 24, :] = total

    def row(which, block):
        at = (block // 12) * 24 + which * 12 + block % 12
        return mods[at : at + 1, :]

    for j in range(16):
        gate_out[j : j + 1, :] = row(0, 32 + j)
    none = jnp.zeros((ROWS - SPAN - CTX_OWN, LANES), F32)
    for which, rows in ((0, slice(0, SPAN)), (1, slice(SPAN, ROWS))):
        for j in range(16):
            cols = slice(j * LANES, (j + 1) * LANES)
            if which == 0:
                values = latent[0, :, cols].astype(F32)
            else:
                values = jnp.concatenate([context[0, :, cols].astype(F32), none], axis=0)
            scale = gain[j : j + 1, :].astype(F32) * (1.0 + row(which, 16 + j))
            tile = values * factors[rows, :] * scale + row(which, j)
            rows_in[rows, cols] = tile.astype(BF16)
    inputs = rows_in[...]

    def heads(values):
        return [values[:, h * HEAD : (h + 1) * HEAD] for h in range(2)]

    added, rate, bias = (consts[n : n + 4, :ROWS] for n in (0, 4, 8))
    small = rounded(dot(w_small[...], inputs, ((1,), (1,))))
    decay_raw, beta_raw = small[:4], small[4:]
    pre = decay_raw + bias
    soft = jnp.maximum(pre, 0.0) + jnp.log1p(jnp.exp(-jnp.abs(pre)))
    log_decay = -rate * soft + added
    beta = BETA_SCALE * rate / (1.0 + jnp.exp(-beta_raw))
    pad = jnp.zeros((4, 256 - ROWS), F32)
    g_high, g_low = split_in_two(jnp.concatenate([log_decay, pad], axis=1))
    b_high, b_low = split_in_two(jnp.concatenate([beta, pad], axis=1))

    def unit(v):
        return v * lax.rsqrt(jnp.sum(v * v, axis=-1, keepdims=True) + NORM_EPS)

    keys = heads(silu(rounded(dot(inputs, w_key[...]))))
    values = heads(silu(rounded(dot(inputs, w_value[...]))))
    copies[0].wait()
    queries = heads(silu(rounded(dot(inputs[:SPAN], w_query[...]))))
    copies[1].wait()
    gates = heads(silu(rounded(dot(inputs[:SPAN], w_gate[...]))))
    low_lanes = iota((ROWS, LANES), 1) < 64
    for h in range(2):
        key = unit(keys[h]).astype(BF16)
        query = (unit(queries[h]) * HEAD**-0.5).astype(BF16)
        gate = jnp.concatenate([gates[h], jnp.zeros((ROWS - SPAN, HEAD), F32)], axis=0)
        small_parts = [v[2 * d + h : 2 * d + h + 1] for d in range(2)
                       for v in (g_high, g_low, b_high, b_low)]
        eight = jnp.concatenate(small_parts, axis=0)
        eight = jnp.concatenate([eight[:, :LANES], eight[:, LANES:]], axis=0).astype(BF16)
        for half in range(2):
            peer = 2 * h + half
            out[peer, K_AT:V_AT, :] = key
            if half == 0:
                both = jnp.where(low_lanes, values[h], pltpu.roll(gate, 64, 1))
            else:
                both = jnp.where(low_lanes, pltpu.roll(values[h], 64, 1), gate)
            out[peer, V_AT:Q_AT, :] = both.astype(BF16)
            out[peer, Q_AT:S_AT, :] = query
            out[peer, S_AT:X_ROWS, :] = eight


def blocks_apart():
    lane = iota((64, 256), 1) // 64
    return [jnp.where(lane == b, 1.0, 0.0).astype(BF16) for b in range(4)]


def packed_inverses(lows):
    i, j = iota((64, 256), 0), iota((64, 256), 1) % 64
    lanes = blocks_apart()

    def spread(x):
        x = x.astype(BF16)
        return jnp.concatenate([x * mask for mask in lanes], axis=0)

    def times(xs, ys):
        return [dot(x.astype(BF16), y) for x, y in zip(xs, ys)]

    results = None
    for width in (1, 4, 16):
        coupled = (i // (4 * width) == j // (4 * width)) & (i // width != j // width)
        rest = [jnp.where(coupled, low, 0.0) for low in lows]
        if results is None:
            unit = jnp.where(i == j, 1.0, 0.0)
            moves = rest
            first = [unit - m for m in moves]
            squares = times(moves, [spread(m) for m in moves])
        else:
            moves = times(results, [spread(r) for r in rest])
            spreads = [spread(r) for r in results]
            squares = times(moves, [spread(m) for m in moves])
            first = [r - p for r, p in zip(results, times(moves, spreads))]
        second = times(squares, [spread(q) for q in first])
        results = [q + p for q, p in zip(first, second)]
    return results


def pack(low):
    lane = iota((64, LANES), 1) < 64
    tiles = []
    for t in range(2):
        tile = low[LANES * t : LANES * t + LANES, LANES * t : LANES * t + LANES]
        tiles.append(jnp.where(lane, tile[:64], tile[64:]))
    return jnp.concatenate(tiles, axis=1)


def unpack(packed):
    lanes = blocks_apart()
    return jnp.concatenate([packed * mask.astype(F32) for mask in lanes], axis=0)


def widened(results, lows, width, times):
    i, j = iota((CHUNK, CHUNK), 0), iota((CHUNK, CHUNK), 1)
    wide = times * width
    coupled = (i // wide == j // wide) & (i // width != j // width)
    half = [r.astype(BF16) for r in results]
    moves = [
        dot(r, jnp.where(coupled, low, 0.0).astype(BF16)).astype(BF16)
        for r, low in zip(half, lows)
    ]
    squares = [dot(m, m).astype(BF16) for m in moves] if times == 4 else None
    first = [r - dot(m, h) for r, m, h in zip(results, moves, half)]
    if times == 2:
        return first
    return [q + dot(m, q.astype(BF16)) for q, m in zip(first, squares)]


class Order:
    def __init__(self, n):
        self.away = iota((n, n), 0) - iota((n, n), 1)
        self.same = jnp.where(self.away == 0, 1.0, 0.0).astype(BF16)
        self.upto = [
            jnp.where(a >= 0, 1.0, 0.0).astype(BF16) for a in (self.away, -self.away)
        ]

    def block(self, key, rows):
        n = key.shape[0]
        pairs = dot(key, key, ((1,), (1,)))
        rates = dot(self.same, rows, ((1,), (1,)))
        key32 = key.astype(F32)
        found = []
        for d in range(2):
            sums = dot(self.upto[d], rows, ((1,), (1,)))
            down = sums[:, 4 * d : 4 * d + 1] + sums[:, 4 * d + 1 : 4 * d + 2]
            across = dot(rows, self.upto[d], ((1,), (1,)))
            along = across[4 * d : 4 * d + 1] + across[4 * d + 1 : 4 * d + 2]
            reach = self.away if d == 0 else -self.away
            weights = jnp.where(reach >= 0, jnp.exp(jnp.where(reach >= 0, down - along, 0.0)), 0.0)
            beta = rates[:, 4 * d + 2 : 4 * d + 3] + rates[:, 4 * d + 3 : 4 * d + 4]
            total = down[n - 1 : n] if d == 0 else down[0:1]
            low = jnp.where(reach > 0, pairs * weights * beta, 0.0)
            kept = (key32 * jnp.exp(total - down)).astype(BF16)
            found.append((low, beta, jnp.exp(down), kept, jnp.exp(total), weights))
        return found


def small_rows(got):
    low_lanes = iota((8, LANES), 1) < 64
    small = [got[p, S_AT:X_ROWS, :].astype(F32) for p in range(4)]
    first = [s[:8] for s in small]
    second = [s[8:] for s in small]
    turn = lambda v: pltpu.roll(v, 64, 1)
    blocks = [
        first[0],
        jnp.where(low_lanes, second[0], turn(first[1])),
        jnp.where(low_lanes, turn(first[1]), turn(second[1])),
        first[2],
        jnp.where(low_lanes, second[2], turn(first[3])),
        jnp.where(low_lanes, turn(first[3]), turn(second[3])),
    ]
    lane = iota((8, LANES), 1)
    ctx_small = jnp.zeros((8, LANES), F32)
    for p in range(4):
        here = (lane >= 8 * p) & (lane < 8 * p + 8)
        ctx_small = jnp.where(here, pltpu.roll(second[p], (64 + 8 * p) % 128, 1), ctx_small)
    rows = [
        jnp.concatenate([blocks[2 * m], blocks[2 * m + 1]], axis=1).astype(BF16)
        for m in range(CHUNKS)
    ]
    return rows, ctx_small


def latent_rows(got, at, m):
    pieces = {
        0: ((0, 0, 192), (1, 0, 64)),
        1: ((1, 64, 192), (2, 0, 128)),
        2: ((2, 128, 192), (3, 0, 192)),
    }[m]
    return jnp.concatenate([got[p, at + a : at + b, :] for p, a, b in pieces], axis=0)


def add_block(mine, so_far):
    nxt = dot(mine[:, HEAD:].astype(BF16), so_far.astype(BF16))
    return jnp.concatenate([nxt[:, :HEAD] + mine[:, :HEAD].astype(F32), nxt[:, HEAD:]], axis=1)


def token_maps(got, out, reads, offsets, weights_of, maps):
    order = Order(CHUNK)

    def ctx_rows(at):
        return jnp.concatenate(
            [got[p, at + SPAN : at + ROWS, :].astype(F32)[:CTX_OWN] for p in range(4)], axis=0
        )

    rows, ctx_small = small_rows(got)
    keys = [latent_rows(got, K_AT, m) for m in range(CHUNKS)]
    values = [latent_rows(got, V_AT, m).astype(F32) for m in range(CHUNKS)]
    ctx_key, ctx_value = ctx_rows(K_AT), ctx_rows(V_AT)
    padded = jnp.concatenate([ctx_key, jnp.zeros((LANES - 32, HEAD), F32)], axis=0).astype(BF16)
    ctx_lows = [f[0] for f in Order(LANES).block(padded, ctx_small.astype(BF16))]
    left = iota((64, LANES), 1) < 64
    ctx_low = jnp.concatenate(
        [
            jnp.where(left, ctx_lows[0][:64], pltpu.roll(ctx_lows[1][:64], 64, 1)),
            jnp.zeros((64, LANES), F32),
        ],
        axis=1,
    )
    lows, rights, kept, totals, decays = [], [], [], [], []
    for m in range(CHUNKS):
        for d, (low, beta, decayed, keep, total, weights) in enumerate(
            order.block(keys[m], rows[m])
        ):
            lows.append(low)
            key = keys[m].astype(F32) * (beta * decayed)
            rights.append(jnp.concatenate([values[m] * beta, key], axis=1).astype(BF16))
            kept.append(keep)
            totals.append(total)
            decays.append(decayed)
            weights_of[2 * m + d] = weights
    packed = packed_inverses([pack(low) for low in lows] + [ctx_low])
    inverses = widened([unpack(p) for p in packed[:-1]], lows, 64, 4)
    factors = [dot(t.astype(BF16), r).astype(BF16) for t, r in zip(inverses, rights)]
    unit = jnp.where(iota((HEAD, HEAD), 0) == iota((HEAD, HEAD), 1), 1.0, 0.0)
    for n in range(2 * CHUNKS):
        both = dot(kept[n], factors[n], ((0,), (0,)))
        maps[n] = jnp.concatenate([both[:, :HEAD], totals[n] * unit - both[:, HEAD:]], axis=1)

    so_far = [None, None]
    passed = [[None] * CHUNKS for _ in range(2)]
    for step in range(CHUNKS):
        for d in range(2):
            m = step if d == 0 else CHUNKS - 1 - step
            passed[d][m] = so_far[d]
            mine = maps[2 * m + d]
            so_far[d] = mine if step == 0 else add_block(mine, so_far[d])
    for m in range(CHUNKS):
        query = latent_rows(got, Q_AT, m)
        pairs = dot(query, keys[m], ((1,), (1,)))
        at = slice(m * CHUNK, (m + 1) * CHUNK)
        offset = None
        for d in range(2):
            n = 2 * m + d
            local = dot((pairs * weights_of[n]).astype(BF16), factors[n])
            read = (query.astype(F32) * decays[n] - local[:, HEAD:]).astype(BF16)
            mine = local[:, :HEAD]
            if passed[d][m] is not None:
                moved = dot(read, passed[d][m].astype(BF16))
                read, mine = moved[:, HEAD:].astype(BF16), mine + moved[:, :HEAD]
            reads[at, d * HEAD : (d + 1) * HEAD] = read
            offset = mine if offset is None else offset + mine
        offsets[at, :] = offset

    ctx_inverse = packed[-1][:32, :LANES]
    merged = ctx_inverse + pltpu.roll(ctx_inverse, 64, 1)
    merged = merged - jnp.where(iota((32, LANES), 0) == iota((32, LANES), 1), 1.0, 0.0)
    narrow = iota((16, LANES), 1) < 96
    turn = lambda v: pltpu.roll(v, 64, 1)
    spare = jnp.concatenate(
        [
            turn(ctx_key), ctx_key, turn(ctx_value), turn(ctx_small),
            jnp.where(narrow, turn(merged[:16]), pltpu.roll(merged[16:], 96, 1)),
            jnp.zeros((8, LANES), F32),
        ],
        axis=0,
    )
    left = iota((HEAD, LANES), 1) < 64
    whole = [
        jnp.concatenate([jnp.where(left, m[:, :HEAD], spare), m[:, HEAD:]], axis=1) for m in so_far
    ]
    place = lax.axis_index("z")
    for k in range(out.shape[0]):
        out[k] = jnp.where(k > place, whole[0], whole[1]).astype(BF16)


def read_states(got, reads, offsets, sent, out):
    count = got.shape[0]
    place = lax.axis_index("z")
    turn = lambda v: pltpu.roll(v, 64, 1)
    unit = jnp.where(iota((HEAD, HEAD), 0) == iota((HEAD, HEAD), 1), 1.0, 0.0)
    left = iota((32, LANES), 1) < 64
    lane = iota((16, LANES), 1)
    key, value, starts = [], [], []
    rows = [jnp.zeros((8, LANES), F32)] * 2
    none = jnp.zeros((16, LANES), F32)
    for k in range(count):
        spare = got[k, :, :LANES].astype(F32)
        key.append(jnp.where(left, turn(spare[:32]), spare[32:64]))
        value.append(turn(spare[64:96]))
        here = lane // 32 == k % 4
        at = 32 * (k % 4)
        rows[k // 4] = jnp.where(
            here[:8], pltpu.roll(spare[96:104], (at - 64) % LANES, 1), rows[k // 4]
        )
        for shift in (64, 96):
            one = jnp.where(here, pltpu.roll(spare[104:120], (at - shift) % LANES, 1), 0.0)
            starts.append(jnp.concatenate([one, none] if k < 4 else [none, one], axis=1))
    key = jnp.concatenate(key, axis=0).astype(BF16)
    value = jnp.concatenate(value, axis=0)
    start = jnp.concatenate(starts, axis=0)
    order = Order(CHUNK)
    found = order.block(key, jnp.concatenate(rows, axis=1).astype(BF16))
    lows = [f[0] for f in found]
    whole = jnp.where(order.away == 0, 1.0, 0.0)
    results = [jnp.where(a > 0, start, whole) for a in (order.away, -order.away)]
    inverses = widened(widened(results, lows, 32, 4), lows, 128, 2)
    ctx_states = []
    for inverse, (_, beta, _, kept, _, _) in zip(inverses, found):
        fresh = dot(inverse.astype(BF16), (value * beta).astype(BF16))
        ctx_states.append(dot(kept, fresh.astype(BF16), ((0,), (0,))))

    chains = [jnp.concatenate([jnp.zeros((HEAD, HEAD), F32), unit], axis=1)] * 2
    for step in range(count - 1):
        for d in range(2):
            k = step if d == 0 else count - 1 - step
            used = k < place if d == 0 else k > place
            chains[d] = jnp.where(used, add_block(got[k], chains[d]), chains[d])
    states = [
        (dot(c[:, HEAD:].astype(BF16), s.astype(BF16)) + c[:, :HEAD]).astype(BF16)
        for c, s in zip(chains, ctx_states)
    ]
    state = jnp.concatenate(states, axis=0)
    left = iota((48, LANES), 1) < 64
    for x in range(4):
        at = slice(SPAN * x, SPAN * x + SPAN)
        o = dot(reads[at, :], state) + offsets[at, :]
        gates = sent[x, V_AT : V_AT + SPAN, :].astype(F32)
        for y in range(4):
            own = slice(48 * y, 48 * y + 48)
            out[4 * x + y] = jnp.where(left, o[own], gates[own]).astype(BF16)


def mix(got, out_gain, gate, w_out, latent, out):
    left = iota((48, LANES), 1) < 64
    gain = out_gain[...].astype(F32)
    tiles = []
    for y in range(4):
        for h in range(2):
            one = got[8 * h + y].astype(F32)
            two = got[8 * h + 4 + y].astype(F32)
            o = jnp.where(left, one, pltpu.roll(two, 64, 1))
            gates = jnp.where(left, pltpu.roll(one, 64, 1), two)
            normed = o * lax.rsqrt(jnp.mean(o * o, axis=-1, keepdims=True) + NORM_EPS)
            tiles.append((normed * gain * gates).astype(BF16))
    gated = jnp.concatenate(tiles, axis=1)
    start = pl.multiple_of(lax.axis_index("tp") * 48, 16)
    own = latent[pl.ds(start, 48), :].astype(F32)
    for n in range(0, D, 512):
        mixed = dot(gated, w_out[:, n : n + 512])
        for c in range(0, 512, LANES):
            j = (n + c) // LANES
            cols = slice(n + c, n + c + LANES)
            out[:, cols] = (own[:, cols] + gate[j : j + 1, :] * mixed[:, c : c + LANES]).astype(BF16)


VM = pl.BlockSpec(memory_space=pltpu.VMEM)


HBM = pl.BlockSpec(memory_space=pltpu.HBM)


def call(body, name, n_in, outs, scratch=(), mib=16, n_hbm=0):
    many = isinstance(outs, (list, tuple))
    return pl.pallas_call(
        body,
        out_shape=outs,
        in_specs=[VM] * n_in + [HBM] * n_hbm,
        out_specs=[VM] * len(outs) if many else VM,
        scratch_shapes=list(scratch),
        compiler_params=pltpu.CompilerParams(vmem_limit_bytes=mib << 20),
        name=name,
    )


def shape(dims, dtype=BF16):
    return jax.ShapeDtypeStruct(dims, dtype)


def in_hbm(array):
    return pltpu.with_memory_space_constraint(array, pltpu.HBM)


def swap(array, axes):
    return lax.all_to_all(array, axes, 0, 0, tiled=True)


def on_device(
    latent, cond, context, ctx_cond, w_mod, norm_gain, w_query, w_key, w_value, w_outgate,
    w_decay, w_beta, decay_rate, decay_bias, extra_decay, out_gain, w_out,
):
    by_row = lambda w: w.transpose(1, 2, 0)
    fetched = (
        norm_gain.reshape(16, LANES), by_row(w_decay), by_row(w_beta), decay_rate, decay_bias,
        extra_decay, latent, context, w_key, w_value,
    )
    space = lambda n: pltpu.SMEM if n in (3, 4) else pltpu.VMEM
    prepared = call(
        prepare, "prepare", 0,
        [shape(w.shape) for w in fetched[8:]]
        + [
            shape(latent.shape), shape(context.shape), shape((ROWS, LANES), F32),
            shape((16, LANES)), shape((8, D)), shape((16, 256), F32),
        ],
        [space(n)(a.shape, a.dtype) for n, a in enumerate(fetched) if 1 <= n <= 5]
        + [pltpu.SemaphoreType.DMA((len(fetched),))],
        16, len(fetched),
    )(*(in_hbm(a) for a in fetched))
    partial = call(
        partial_modulation, "partial_modulation", 0, shape((8, 24, LANES)),
        [
            pltpu.VMEM((24, LANES), F32), pltpu.VMEM(cond.shape, BF16),
            pltpu.VMEM(cond.shape, BF16), pltpu.VMEM(w_mod.shape, BF16),
            pltpu.SemaphoreType.DMA((3,)),
        ],
        16, 3,
    )(in_hbm(cond), in_hbm(ctx_cond[None, :]), in_hbm(w_mod))
    summed = call(sum_and_spread, "sum_and_spread", 1, shape((16, 24, LANES)))(swap(partial, "z"))
    parts = swap(summed, ("x", "tp"))
    sent, gate = call(
        project, "project", 1 + len(prepared), [shape((4, X_ROWS, LANES)), shape((16, LANES), F32)],
        [pltpu.VMEM((96, LANES), F32), pltpu.VMEM((ROWS, D), BF16)]
        + [pltpu.VMEM(w_query.shape, BF16)] * 2 + [pltpu.SemaphoreType.DMA((2,))],
        24, 2,
    )(parts, *prepared, in_hbm(w_query), in_hbm(w_outgate))
    held = swap(sent, "x")
    maps, reads, offsets = call(
        token_maps, "token_maps", 1,
        [shape((8, HEAD, 256)), shape((ROW_OF_X, 256)), shape((ROW_OF_X, HEAD), F32)],
        [
            pltpu.VMEM((2 * CHUNKS, CHUNK, CHUNK), F32), pltpu.VMEM((2 * CHUNKS, HEAD, 256), F32),
        ],
    )(held)
    reached = swap(maps, "z")
    outs = call(read_states, "read_states", 4, shape((16, 48, LANES)))(
        reached, reads, offsets, held
    )
    gathered = swap(outs, ("x", "tp"))
    mixed = call(mix, "mix", 5, shape((48, D)))(
        gathered, out_gain[None, :], gate, w_out, latent[0]
    )
    return mixed[None]


def solution(mesh):
    torus = Mesh(
        mesh.devices.reshape(8, 4, mesh.shape["tp"], mesh.shape["dp"]), ("z", "x", "tp", "dp")
    )
    sp = ("z", "x")
    return jax.shard_map(
        on_device,
        mesh=torus,
        in_specs=(
            P("dp", sp, None),
            P("dp", sp),
            P("dp", sp, None),
            P(sp),
            P(sp, "tp"),
            P(),
            P(None, "tp"),
            P(None, "tp"),
            P(None, "tp"),
            P(None, "tp"),
            P(None, None, "tp"),
            P(None, None, "tp"),
            P(None, "tp"),
            P(None, "tp"),
            P("dp", None, "tp", sp),
            P(),
            P(),
        ),
        out_specs=P("dp", ("z", "x", "tp"), None),
        check_vma=False,
    )
```

```python
import functools

import jax
import jax.numpy as jnp
from jax import lax
from jax.experimental import pallas as pl
from jax.experimental.pallas import tpu as pltpu
from jax.sharding import Mesh
from jax.sharding import PartitionSpec as P

D = 2048
HEAD = 128
LANES = 128
NORM_EPS = 1e-06
BETA_SCALE = 30.0

SPAN = 192
CTX_OWN = 8
ROWS = 208
CHUNK = 256
CHUNKS = 3
ROW_OF_X = 4 * SPAN

K_AT, V_AT, Q_AT, S_AT, X_ROWS = 0, 208, 416, 608, 624

FLOPS = 10**10

F32 = jnp.float32
BF16 = jnp.bfloat16


def dot(a, b, dims=((1,), (0,))):
    return lax.dot_general(a, b, (dims, ((), ())), preferred_element_type=F32)


def silu(v):
    return v / (1.0 + jnp.exp(-v))


def rounded(v):
    return v.astype(BF16).astype(F32)


def split_in_two(v):
    high = v.astype(BF16)
    return high.astype(F32), v - high.astype(F32)


def iota(shape, dim):
    return lax.broadcasted_iota(jnp.int32, shape, dim)


def fetch(pairs, sems):
    copies = [pltpu.make_async_copy(a, b, sems.at[n]) for n, (a, b) in enumerate(pairs)]
    for copy in copies:
        copy.start()
    return copies


def partial_modulation(cond_in, ctx_cond_in, w_mod_in, out, rows, cond, ctx_cond, w_mod, sems):
    pairs = ((w_mod_in, w_mod), (cond_in, cond), (ctx_cond_in, ctx_cond))
    for copy in fetch(pairs, sems):
        copy.wait()
    first = iota((8, cond.shape[1]), 0) == 0
    values = jnp.where(first, cond[...].astype(F32), ctx_cond[...].astype(F32))
    product = dot(silu(values).astype(BF16), w_mod[...])
    for r in range(2):
        for c in range(12):
            rows[r * 12 + c : r * 12 + c + 1, :] = product[r : r + 1, c * LANES : (c + 1) * LANES]
    value = rows[...].astype(BF16)
    for k in range(out.shape[0]):
        out[k] = value


def sum_and_spread(parts, out):
    total = parts[0].astype(F32)
    for k in range(1, parts.shape[0]):
        total = total + parts[k].astype(F32)
    value = total.astype(BF16)
    for k in range(out.shape[0]):
        out[k] = value


def project(
    parts, gain, latent, context, w_key, w_value, w_query, w_gate,
    decay_in, beta_in, rate_in, bias_in, extra_in,
    out, gate_out, mods, rows_in, w_decay, w_beta, rate_at, bias_at, extra, sems,
):
    copies = fetch(
        (
            (decay_in, w_decay), (beta_in, w_beta), (rate_in, rate_at), (bias_in, bias_at),
            (extra_in, extra),
        ),
        sems,
    )
    for y in range(4):
        total = parts[y].astype(F32)
        for x in range(1, 4):
            total = total + parts[4 * x + y].astype(F32)
        mods[24 * y : 24 * y + 24, :] = total

    def row(which, block):
        at = (block // 12) * 24 + which * 12 + block % 12
        return mods[at : at + 1, :]

    for j in range(16):
        gate_out[j : j + 1, :] = row(0, 32 + j)

    def modulate(values, which, at):
        factor = lax.rsqrt(jnp.mean(values * values, axis=-1, keepdims=True) + NORM_EPS)
        for j in range(16):
            cols = slice(j * LANES, (j + 1) * LANES)
            scale = gain[j : j + 1, :].astype(F32) * (1.0 + row(which, 16 + j))
            tile = values[:, cols] * factor * scale + row(which, j)
            rows_in[at : at + values.shape[0], cols] = tile.astype(BF16)

    for g in range(0, SPAN, 64):
        modulate(latent[0, g : g + 64, :].astype(F32), 0, g)
    none = jnp.zeros((ROWS - SPAN - CTX_OWN, D), F32)
    modulate(jnp.concatenate([context[0].astype(F32), none], axis=0), 1, SPAN)
    inputs = rows_in[...]

    def heads(values):
        return [values[:, h * HEAD : (h + 1) * HEAD] for h in range(2)]

    def unit(v):
        return v * lax.rsqrt(jnp.sum(v * v, axis=-1, keepdims=True) + NORM_EPS)

    keys = heads(silu(rounded(dot(inputs, w_key[...]))))
    values = heads(silu(rounded(dot(inputs, w_value[...]))))
    queries = heads(silu(rounded(dot(inputs[:SPAN], w_query[...]))))
    gates = heads(silu(rounded(dot(inputs[:SPAN], w_gate[...]))))
    for copy in copies:
        copy.wait()

    def column(at):
        row = iota((4, 1), 0)
        value = jnp.where(row == 0, at[0, 0], at[0, 1])
        return jnp.where(row < 2, value, jnp.where(row == 2, at[1, 0], at[1, 1]))

    rate, bias = column(rate_at), column(bias_at)
    w_small = jnp.concatenate(
        [w[d].astype(F32) for w in (w_decay, w_beta) for d in range(2)], axis=0
    ).astype(BF16)
    latent_only = jnp.concatenate([extra[0, 0], extra[0, 1]], axis=0)
    added = jnp.concatenate([latent_only, jnp.zeros((4, ROWS - SPAN), F32)], axis=1)
    small = rounded(dot(w_small, inputs, ((1,), (1,))))
    decay_raw, beta_raw = small[:4], small[4:]
    pre = decay_raw + bias
    soft = jnp.maximum(pre, 0.0) + jnp.log1p(jnp.exp(-jnp.abs(pre)))
    log_decay = -rate * soft + added
    beta = BETA_SCALE * rate / (1.0 + jnp.exp(-beta_raw))
    pad = jnp.zeros((4, 256 - ROWS), F32)
    g_high, g_low = split_in_two(jnp.concatenate([log_decay, pad], axis=1))
    b_high, b_low = split_in_two(jnp.concatenate([beta, pad], axis=1))

    low_lanes = iota((ROWS, LANES), 1) < 64
    for h in range(2):
        key = unit(keys[h]).astype(BF16)
        query = (unit(queries[h]) * HEAD**-0.5).astype(BF16)
        gate = jnp.concatenate([gates[h], jnp.zeros((ROWS - SPAN, HEAD), F32)], axis=0)
        small_parts = [v[2 * d + h : 2 * d + h + 1] for d in range(2)
                       for v in (g_high, g_low, b_high, b_low)]
        eight = jnp.concatenate(small_parts, axis=0)
        eight = jnp.concatenate([eight[:, :LANES], eight[:, LANES:]], axis=0).astype(BF16)
        for half in range(2):
            peer = 2 * h + half
            out[peer, K_AT:V_AT, :] = key
            if half == 0:
                both = jnp.where(low_lanes, values[h], pltpu.roll(gate, 64, 1))
            else:
                both = jnp.where(low_lanes, pltpu.roll(values[h], 64, 1), gate)
            out[peer, V_AT:Q_AT, :] = both.astype(BF16)
            out[peer, Q_AT:S_AT, :] = query
            out[peer, S_AT:X_ROWS, :] = eight


def blocks_apart():
    lane = iota((64, 256), 1) // 64
    return [jnp.where(lane == b, 1.0, 0.0).astype(BF16) for b in range(4)]


def packed_inverses(lows):
    i, j = iota((64, 256), 0), iota((64, 256), 1) % 64
    lanes = blocks_apart()

    def spread(x):
        x = x.astype(BF16)
        return jnp.concatenate([x * mask for mask in lanes], axis=0)

    def times(xs, ys):
        return [dot(x.astype(BF16), y) for x, y in zip(xs, ys)]

    results = None
    for width in (1, 4, 16):
        coupled = (i // (4 * width) == j // (4 * width)) & (i // width != j // width)
        rest = [jnp.where(coupled, low, 0.0) for low in lows]
        if results is None:
            unit = jnp.where(i == j, 1.0, 0.0)
            moves = rest
            first = [unit - m for m in moves]
            squares = times(moves, [spread(m) for m in moves])
        else:
            moves = times(results, [spread(r) for r in rest])
            spreads = [spread(r) for r in results]
            squares = times(moves, [spread(m) for m in moves])
            first = [r - p for r, p in zip(results, times(moves, spreads))]
        second = times(squares, [spread(q) for q in first])
        results = [q + p for q, p in zip(first, second)]
    return results


def pack(low):
    lane = iota((64, LANES), 1) < 64
    tiles = []
    for t in range(2):
        tile = low[LANES * t : LANES * t + LANES, LANES * t : LANES * t + LANES]
        tiles.append(jnp.where(lane, tile[:64], tile[64:]))
    return jnp.concatenate(tiles, axis=1)


def unpack(packed):
    lanes = blocks_apart()
    return jnp.concatenate([packed * mask.astype(F32) for mask in lanes], axis=0)


def widened(results, lows, width, times):
    i, j = iota((CHUNK, CHUNK), 0), iota((CHUNK, CHUNK), 1)
    wide = times * width
    coupled = (i // wide == j // wide) & (i // width != j // width)
    half = [r.astype(BF16) for r in results]
    moves = [
        dot(r, jnp.where(coupled, low, 0.0).astype(BF16)).astype(BF16)
        for r, low in zip(half, lows)
    ]
    squares = [dot(m, m).astype(BF16) for m in moves] if times == 4 else None
    first = [r - dot(m, h) for r, m, h in zip(results, moves, half)]
    if times == 2:
        return first
    return [q + dot(m, q.astype(BF16)) for q, m in zip(first, squares)]


class Order:
    def __init__(self, n):
        self.away = iota((n, n), 0) - iota((n, n), 1)
        self.same = jnp.where(self.away == 0, 1.0, 0.0).astype(BF16)
        self.upto = [
            jnp.where(a >= 0, 1.0, 0.0).astype(BF16) for a in (self.away, -self.away)
        ]

    def block(self, key, rows):
        n = key.shape[0]
        pairs = dot(key, key, ((1,), (1,)))
        rows32 = rows.astype(F32)
        key32 = key.astype(F32)

        def down_columns(matrix, at):
            two = [jnp.broadcast_to(rows32[r : r + 1], (LANES, n)) for r in (at, at + 1)]
            both = dot(matrix, jnp.concatenate(two, axis=0).astype(BF16), ((1,), (1,)))
            return both[:, :LANES] + both[:, LANES:]

        wide = lambda v: jnp.concatenate([v] * (n // LANES), axis=1)
        found = []
        for d in range(2):
            down = down_columns(self.upto[d], 4 * d)
            beta = down_columns(self.same, 4 * d + 2)
            across = dot(rows, self.upto[1 - d])
            along = across[4 * d : 4 * d + 1] + across[4 * d + 1 : 4 * d + 2]
            reach = self.away if d == 0 else -self.away
            weights = jnp.where(
                reach >= 0, jnp.exp(jnp.where(reach >= 0, wide(down) - along, 0.0)), 0.0
            )
            total = down[n - 1 : n] if d == 0 else down[0:1]
            low = jnp.where(reach > 0, pairs * weights * wide(beta), 0.0)
            kept = (key32 * jnp.exp(total - down)).astype(BF16)
            found.append((low, beta, jnp.exp(down), kept, jnp.exp(total), weights))
        return found


def small_rows(got):
    low_lanes = iota((8, LANES), 1) < 64
    small = [got[p, S_AT:X_ROWS, :].astype(F32) for p in range(4)]
    first = [s[:8] for s in small]
    second = [s[8:] for s in small]
    turn = lambda v: pltpu.roll(v, 64, 1)
    blocks = [
        first[0],
        jnp.where(low_lanes, second[0], turn(first[1])),
        jnp.where(low_lanes, turn(first[1]), turn(second[1])),
        first[2],
        jnp.where(low_lanes, second[2], turn(first[3])),
        jnp.where(low_lanes, turn(first[3]), turn(second[3])),
    ]
    lane = iota((8, LANES), 1)
    ctx_small = jnp.zeros((8, LANES), F32)
    for p in range(4):
        here = (lane >= 8 * p) & (lane < 8 * p + 8)
        ctx_small = jnp.where(here, pltpu.roll(second[p], (64 + 8 * p) % 128, 1), ctx_small)
    rows = [
        jnp.concatenate([blocks[2 * m], blocks[2 * m + 1]], axis=1).astype(BF16)
        for m in range(CHUNKS)
    ]
    return rows, ctx_small


def latent_rows(got, at, m):
    pieces = {
        0: ((0, 0, 192), (1, 0, 64)),
        1: ((1, 64, 192), (2, 0, 128)),
        2: ((2, 128, 192), (3, 0, 192)),
    }[m]
    return jnp.concatenate([got[p, at + a : at + b, :] for p, a, b in pieces], axis=0)


def add_block(mine, so_far):
    nxt = dot(mine[:, HEAD:].astype(BF16), so_far.astype(BF16))
    return jnp.concatenate([nxt[:, :HEAD] + mine[:, :HEAD].astype(F32), nxt[:, HEAD:]], axis=1)


def token_maps(got, out, reads, offsets, weights_of, maps):
    order = Order(CHUNK)

    def ctx_rows(at):
        return jnp.concatenate(
            [got[p, at + SPAN : at + ROWS, :].astype(F32)[:CTX_OWN] for p in range(4)], axis=0
        )

    rows, ctx_small = small_rows(got)
    keys = [latent_rows(got, K_AT, m) for m in range(CHUNKS)]
    values = [latent_rows(got, V_AT, m).astype(F32) for m in range(CHUNKS)]
    ctx_key, ctx_value = ctx_rows(K_AT), ctx_rows(V_AT)
    padded = jnp.concatenate([ctx_key, jnp.zeros((LANES - 32, HEAD), F32)], axis=0).astype(BF16)
    ctx_lows = [f[0] for f in Order(LANES).block(padded, ctx_small.astype(BF16))]
    left = iota((64, LANES), 1) < 64
    ctx_low = jnp.concatenate(
        [
            jnp.where(left, ctx_lows[0][:64], pltpu.roll(ctx_lows[1][:64], 64, 1)),
            jnp.zeros((64, LANES), F32),
        ],
        axis=1,
    )
    lows, rights, kept, totals, decays = [], [], [], [], []
    for m in range(CHUNKS):
        for d, (low, beta, decayed, keep, total, weights) in enumerate(
            order.block(keys[m], rows[m])
        ):
            lows.append(low)
            key = keys[m].astype(F32) * (beta * decayed)
            rights.append(jnp.concatenate([values[m] * beta, key], axis=1).astype(BF16))
            kept.append(keep)
            totals.append(total)
            decays.append(decayed)
            weights_of[2 * m + d] = weights
    packed = packed_inverses([pack(low) for low in lows] + [ctx_low])
    inverses = widened([unpack(p) for p in packed[:-1]], lows, 64, 4)
    factors = [dot(t.astype(BF16), r).astype(BF16) for t, r in zip(inverses, rights)]
    unit = jnp.where(iota((HEAD, HEAD), 0) == iota((HEAD, HEAD), 1), 1.0, 0.0)
    for n in range(2 * CHUNKS):
        both = dot(kept[n], factors[n], ((0,), (0,)))
        maps[n] = jnp.concatenate([both[:, :HEAD], totals[n] * unit - both[:, HEAD:]], axis=1)

    so_far = [None, None]
    passed = [[None] * CHUNKS for _ in range(2)]
    for step in range(CHUNKS):
        for d in range(2):
            m = step if d == 0 else CHUNKS - 1 - step
            passed[d][m] = so_far[d]
            mine = maps[2 * m + d]
            so_far[d] = mine if step == 0 else add_block(mine, so_far[d])
    for m in range(CHUNKS):
        query = latent_rows(got, Q_AT, m)
        pairs = dot(query, keys[m], ((1,), (1,)))
        at = slice(m * CHUNK, (m + 1) * CHUNK)
        offset = None
        for d in range(2):
            n = 2 * m + d
            local = dot((pairs * weights_of[n]).astype(BF16), factors[n])
            read = (query.astype(F32) * decays[n] - local[:, HEAD:]).astype(BF16)
            mine = local[:, :HEAD]
            if passed[d][m] is not None:
                moved = dot(read, passed[d][m].astype(BF16))
                read, mine = moved[:, HEAD:].astype(BF16), mine + moved[:, :HEAD]
            reads[at, d * HEAD : (d + 1) * HEAD] = read
            offset = mine if offset is None else offset + mine
        offsets[at, :] = offset

    ctx_inverse = packed[-1][:32, :LANES]
    merged = ctx_inverse + pltpu.roll(ctx_inverse, 64, 1)
    merged = merged - jnp.where(iota((32, LANES), 0) == iota((32, LANES), 1), 1.0, 0.0)
    narrow = iota((16, LANES), 1) < 96
    turn = lambda v: pltpu.roll(v, 64, 1)
    spare = jnp.concatenate(
        [
            turn(ctx_key), ctx_key, turn(ctx_value), turn(ctx_small),
            jnp.where(narrow, turn(merged[:16]), pltpu.roll(merged[16:], 96, 1)),
            jnp.zeros((8, LANES), F32),
        ],
        axis=0,
    )
    left = iota((HEAD, LANES), 1) < 64
    whole = [
        jnp.concatenate([jnp.where(left, m[:, :HEAD], spare), m[:, HEAD:]], axis=1) for m in so_far
    ]
    place = lax.axis_index("z")
    for k in range(out.shape[0]):
        out[k] = jnp.where(k > place, whole[0], whole[1]).astype(BF16)


def read_states(got, reads, offsets, sent, out):
    count = got.shape[0]
    place = lax.axis_index("z")
    turn = lambda v: pltpu.roll(v, 64, 1)
    unit = jnp.where(iota((HEAD, HEAD), 0) == iota((HEAD, HEAD), 1), 1.0, 0.0)
    left = iota((32, LANES), 1) < 64
    lane = iota((16, LANES), 1)
    key, value, starts = [], [], []
    rows = [jnp.zeros((8, LANES), F32)] * 2
    none = jnp.zeros((16, LANES), F32)
    for k in range(count):
        spare = got[k, :, :LANES].astype(F32)
        key.append(jnp.where(left, turn(spare[:32]), spare[32:64]))
        value.append(turn(spare[64:96]))
        here = lane // 32 == k % 4
        at = 32 * (k % 4)
        rows[k // 4] = jnp.where(
            here[:8], pltpu.roll(spare[96:104], (at - 64) % LANES, 1), rows[k // 4]
        )
        for shift in (64, 96):
            one = jnp.where(here, pltpu.roll(spare[104:120], (at - shift) % LANES, 1), 0.0)
            starts.append(jnp.concatenate([one, none] if k < 4 else [none, one], axis=1))
    key = jnp.concatenate(key, axis=0).astype(BF16)
    value = jnp.concatenate(value, axis=0)
    start = jnp.concatenate(starts, axis=0)
    order = Order(CHUNK)
    found = order.block(key, jnp.concatenate(rows, axis=1).astype(BF16))
    lows = [f[0] for f in found]
    whole = jnp.where(order.away == 0, 1.0, 0.0)
    results = [jnp.where(a > 0, start, whole) for a in (order.away, -order.away)]
    inverses = widened(widened(results, lows, 32, 4), lows, 128, 2)
    ctx_states = []
    for inverse, (_, beta, _, kept, _, _) in zip(inverses, found):
        fresh = dot(inverse.astype(BF16), (value * beta).astype(BF16))
        ctx_states.append(dot(kept, fresh.astype(BF16), ((0,), (0,))))

    chains = [jnp.concatenate([jnp.zeros((HEAD, HEAD), F32), unit], axis=1)] * 2
    for step in range(count - 1):
        for d in range(2):
            k = step if d == 0 else count - 1 - step
            used = k < place if d == 0 else k > place
            chains[d] = jnp.where(used, add_block(got[k], chains[d]), chains[d])
    states = [
        (dot(c[:, HEAD:].astype(BF16), s.astype(BF16)) + c[:, :HEAD]).astype(BF16)
        for c, s in zip(chains, ctx_states)
    ]
    state = jnp.concatenate(states, axis=0)
    left = iota((48, LANES), 1) < 64
    for x in range(4):
        at = slice(SPAN * x, SPAN * x + SPAN)
        o = dot(reads[at, :], state) + offsets[at, :]
        gates = sent[x, V_AT : V_AT + SPAN, :].astype(F32)
        for y in range(4):
            own = slice(48 * y, 48 * y + 48)
            out[4 * x + y] = jnp.where(left, o[own], gates[own]).astype(BF16)


def mix(got, out_gain, gate, w_out, latent, out):
    left = iota((48, LANES), 1) < 64
    gain = out_gain[...].astype(F32)
    tiles = []
    for y in range(4):
        for h in range(2):
            one = got[8 * h + y].astype(F32)
            two = got[8 * h + 4 + y].astype(F32)
            o = jnp.where(left, one, pltpu.roll(two, 64, 1))
            gates = jnp.where(left, pltpu.roll(one, 64, 1), two)
            normed = o * lax.rsqrt(jnp.mean(o * o, axis=-1, keepdims=True) + NORM_EPS)
            tiles.append((normed * gain * gates).astype(BF16))
    gated = jnp.concatenate(tiles, axis=1)
    start = pl.multiple_of(lax.axis_index("tp") * 48, 16)
    own = latent[pl.ds(start, 48), :].astype(F32)
    for n in range(0, D, 512):
        mixed = dot(gated, w_out[:, n : n + 512])
        for c in range(0, 512, LANES):
            j = (n + c) // LANES
            cols = slice(n + c, n + c + LANES)
            out[:, cols] = (own[:, cols] + gate[j : j + 1, :] * mixed[:, c : c + LANES]).astype(BF16)


VM = pl.BlockSpec(memory_space=pltpu.VMEM)


HBM = pl.BlockSpec(memory_space=pltpu.HBM)


def call(body, name, n_in, outs, scratch=(), mib=16, n_hbm=0, flops=None):
    many = isinstance(outs, (list, tuple))
    return pl.pallas_call(
        body,
        out_shape=outs,
        in_specs=[VM] * n_in + [HBM] * n_hbm,
        out_specs=[VM] * len(outs) if many else VM,
        scratch_shapes=list(scratch),
        cost_estimate=flops and pl.CostEstimate(flops, 0, 0),
        compiler_params=pltpu.CompilerParams(vmem_limit_bytes=mib << 20),
        name=name,
    )


def shape(dims, dtype=BF16):
    return jax.ShapeDtypeStruct(dims, dtype)


def in_hbm(array):
    return pltpu.with_memory_space_constraint(array, pltpu.HBM)


def swap(array, axes):
    return lax.all_to_all(array, axes, 0, 0, tiled=True)


def on_device(
    latent, cond, context, ctx_cond, w_mod, norm_gain, w_query, w_key, w_value, w_outgate,
    w_decay, w_beta, decay_rate, decay_bias, extra_decay, out_gain, w_out,
):
    partial = call(
        partial_modulation, "partial_modulation", 0, shape((8, 24, LANES)),
        [
            pltpu.VMEM((24, LANES), F32), pltpu.VMEM(cond.shape, BF16),
            pltpu.VMEM(cond.shape, BF16), pltpu.VMEM(w_mod.shape, BF16),
            pltpu.SemaphoreType.DMA((3,)),
        ],
        16, 3, FLOPS,
    )(in_hbm(cond), in_hbm(ctx_cond[None, :]), in_hbm(w_mod))
    summed = call(
        sum_and_spread, "sum_and_spread", 1, shape((16, 24, LANES)), flops=FLOPS
    )(swap(partial, "z"))
    parts = swap(summed, ("x", "tp"))
    by_row = lambda w: w.transpose(1, 2, 0)
    fetched = (by_row(w_decay), by_row(w_beta), decay_rate, decay_bias, extra_decay)
    space = lambda n: pltpu.SMEM if n in (2, 3) else pltpu.VMEM
    sent, gate = call(
        project, "project", 8, [shape((4, X_ROWS, LANES)), shape((16, LANES), F32)],
        [pltpu.VMEM((96, LANES), F32), pltpu.VMEM((ROWS, D), BF16)]
        + [space(n)(a.shape, a.dtype) for n, a in enumerate(fetched)]
        + [pltpu.SemaphoreType.DMA((len(fetched),))],
        16, len(fetched),
    )(
        parts, norm_gain.reshape(16, LANES), latent, context, w_key, w_value, w_query, w_outgate,
        *(in_hbm(a) for a in fetched),
    )
    held = swap(sent, "x")
    maps, reads, offsets = call(
        token_maps, "token_maps", 1,
        [shape((8, HEAD, 256)), shape((ROW_OF_X, 256)), shape((ROW_OF_X, HEAD), F32)],
        [
            pltpu.VMEM((2 * CHUNKS, CHUNK, CHUNK), F32), pltpu.VMEM((2 * CHUNKS, HEAD, 256), F32),
        ],
    )(held)
    reached = swap(maps, "z")
    outs = call(read_states, "read_states", 4, shape((16, 48, LANES)))(
        reached, reads, offsets, held
    )
    gathered = swap(outs, ("x", "tp"))
    mixed = call(mix, "mix", 5, shape((48, D)))(
        gathered, out_gain[None, :], gate, w_out, latent[0]
    )
    return mixed[None]


def solution(mesh):
    torus = Mesh(
        mesh.devices.reshape(8, 4, mesh.shape["tp"], mesh.shape["dp"]), ("z", "x", "tp", "dp")
    )
    sp = ("z", "x")
    return jax.shard_map(
        on_device,
        mesh=torus,
        in_specs=(
            P("dp", sp, None),
            P("dp", sp),
            P("dp", sp, None),
            P(sp),
            P(sp, "tp"),
            P(),
            P(None, "tp"),
            P(None, "tp"),
            P(None, "tp"),
            P(None, "tp"),
            P(None, None, "tp"),
            P(None, None, "tp"),
            P(None, "tp"),
            P(None, "tp"),
            P("dp", None, "tp", sp),
            P(),
            P(),
        ),
        out_specs=P("dp", ("z", "x", "tp"), None),
        check_vma=False,
    )
```

```python
import functools

import jax
import jax.numpy as jnp
from jax import lax
from jax.experimental import pallas as pl
from jax.experimental.pallas import tpu as pltpu
from jax.sharding import Mesh
from jax.sharding import PartitionSpec as P

D = 2048
HEAD = 128
LANES = 128
NORM_EPS = 1e-06
BETA_SCALE = 30.0

SPAN = 192
CTX_OWN = 8
ROWS = 208
CHUNK = 256
CHUNKS = 3
ROW_OF_X = 4 * SPAN

K_AT, V_AT, Q_AT, S_AT, X_ROWS = 0, 208, 416, 608, 624

FLOPS = 10**10

F32 = jnp.float32
BF16 = jnp.bfloat16


def dot(a, b, dims=((1,), (0,))):
    return lax.dot_general(a, b, (dims, ((), ())), preferred_element_type=F32)


def silu(v):
    return v / (1.0 + jnp.exp(-v))


def rounded(v):
    return v.astype(BF16).astype(F32)


def split_in_two(v):
    high = v.astype(BF16)
    return high.astype(F32), v - high.astype(F32)


def iota(shape, dim):
    return lax.broadcasted_iota(jnp.int32, shape, dim)


def fetch(pairs, sems):
    copies = [pltpu.make_async_copy(a, b, sems.at[n]) for n, (a, b) in enumerate(pairs)]
    for copy in copies:
        copy.start()
    return copies


def partial_modulation(cond_in, ctx_cond_in, w_mod_in, out, rows, cond, ctx_cond, w_mod, sems):
    pairs = ((w_mod_in, w_mod), (cond_in, cond), (ctx_cond_in, ctx_cond))
    for copy in fetch(pairs, sems):
        copy.wait()
    first = iota((8, cond.shape[1]), 0) == 0
    values = jnp.where(first, cond[...].astype(F32), ctx_cond[...].astype(F32))
    product = dot(silu(values).astype(BF16), w_mod[...])
    for r in range(2):
        for c in range(12):
            rows[r * 12 + c : r * 12 + c + 1, :] = product[r : r + 1, c * LANES : (c + 1) * LANES]
    value = rows[...].astype(BF16)
    for k in range(out.shape[0]):
        out[k] = value


def sum_and_spread(parts, out):
    total = parts[0].astype(F32)
    for k in range(1, parts.shape[0]):
        total = total + parts[k].astype(F32)
    value = total.astype(BF16)
    for k in range(out.shape[0]):
        out[k] = value


def project(
    parts, gain, latent, context, w_key, w_value, w_query, w_gate,
    w_decay, w_beta, rate_at, bias_at, extra, out, gate_out, mods, rows_in,
):
    for y in range(4):
        total = parts[y].astype(F32)
        for x in range(1, 4):
            total = total + parts[4 * x + y].astype(F32)
        mods[24 * y : 24 * y + 24, :] = total

    def row(which, block):
        at = (block // 12) * 24 + which * 12 + block % 12
        return mods[at : at + 1, :]

    for j in range(16):
        gate_out[j : j + 1, :] = row(0, 32 + j)

    def modulate(values, which, at):
        factor = lax.rsqrt(jnp.mean(values * values, axis=-1, keepdims=True) + NORM_EPS)
        for j in range(16):
            cols = slice(j * LANES, (j + 1) * LANES)
            scale = gain[j : j + 1, :].astype(F32) * (1.0 + row(which, 16 + j))
            tile = values[:, cols] * factor * scale + row(which, j)
            rows_in[at : at + values.shape[0], cols] = tile.astype(BF16)

    for g in range(0, SPAN, 64):
        modulate(latent[0, g : g + 64, :].astype(F32), 0, g)
    none = jnp.zeros((ROWS - SPAN - CTX_OWN, D), F32)
    modulate(jnp.concatenate([context[0].astype(F32), none], axis=0), 1, SPAN)
    inputs = rows_in[...]

    def heads(values):
        return [values[:, h * HEAD : (h + 1) * HEAD] for h in range(2)]

    def unit(v):
        return v * lax.rsqrt(jnp.sum(v * v, axis=-1, keepdims=True) + NORM_EPS)

    keys = heads(silu(rounded(dot(inputs, w_key[...]))))
    values = heads(silu(rounded(dot(inputs, w_value[...]))))
    queries = heads(silu(rounded(dot(inputs[:SPAN], w_query[...]))))
    gates = heads(silu(rounded(dot(inputs[:SPAN], w_gate[...]))))
    def column(at):
        row = iota((4, 1), 0)
        one = jnp.where(row == 0, at[0:1, 0:1], at[0:1, 1:2])
        two = jnp.where(row == 2, at[1:2, 0:1], at[1:2, 1:2])
        return jnp.where(row < 2, one, two)

    rate, bias = column(rate_at), column(bias_at)
    w_small = jnp.concatenate(
        [w[d].astype(F32) for w in (w_decay, w_beta) for d in range(2)], axis=0
    ).astype(BF16)
    latent_only = jnp.concatenate([extra[0, 0], extra[0, 1]], axis=0)
    added = jnp.concatenate([latent_only, jnp.zeros((4, ROWS - SPAN), F32)], axis=1)
    small = rounded(dot(w_small, inputs, ((1,), (1,))))
    decay_raw, beta_raw = small[:4], small[4:]
    pre = decay_raw + bias
    soft = jnp.maximum(pre, 0.0) + jnp.log1p(jnp.exp(-jnp.abs(pre)))
    log_decay = -rate * soft + added
    beta = BETA_SCALE * rate / (1.0 + jnp.exp(-beta_raw))
    pad = jnp.zeros((4, 256 - ROWS), F32)
    g_high, g_low = split_in_two(jnp.concatenate([log_decay, pad], axis=1))
    b_high, b_low = split_in_two(jnp.concatenate([beta, pad], axis=1))

    low_lanes = iota((ROWS, LANES), 1) < 64
    for h in range(2):
        key = unit(keys[h]).astype(BF16)
        query = (unit(queries[h]) * HEAD**-0.5).astype(BF16)
        gate = jnp.concatenate([gates[h], jnp.zeros((ROWS - SPAN, HEAD), F32)], axis=0)
        small_parts = [v[2 * d + h : 2 * d + h + 1] for d in range(2)
                       for v in (g_high, g_low, b_high, b_low)]
        eight = jnp.concatenate(small_parts, axis=0)
        eight = jnp.concatenate([eight[:, :LANES], eight[:, LANES:]], axis=0).astype(BF16)
        for half in range(2):
            peer = 2 * h + half
            out[peer, K_AT:V_AT, :] = key
            if half == 0:
                both = jnp.where(low_lanes, values[h], pltpu.roll(gate, 64, 1))
            else:
                both = jnp.where(low_lanes, pltpu.roll(values[h], 64, 1), gate)
            out[peer, V_AT:Q_AT, :] = both.astype(BF16)
            out[peer, Q_AT:S_AT, :] = query
            out[peer, S_AT:X_ROWS, :] = eight


def blocks_apart():
    lane = iota((64, 256), 1) // 64
    return [jnp.where(lane == b, 1.0, 0.0).astype(BF16) for b in range(4)]


def packed_inverses(lows):
    i, j = iota((64, 256), 0), iota((64, 256), 1) % 64
    lanes = blocks_apart()

    def spread(x):
        x = x.astype(BF16)
        return jnp.concatenate([x * mask for mask in lanes], axis=0)

    def times(xs, ys):
        return [dot(x.astype(BF16), y) for x, y in zip(xs, ys)]

    results = None
    for width in (1, 4, 16):
        coupled = (i // (4 * width) == j // (4 * width)) & (i // width != j // width)
        rest = [jnp.where(coupled, low, 0.0) for low in lows]
        if results is None:
            unit = jnp.where(i == j, 1.0, 0.0)
            moves = rest
            first = [unit - m for m in moves]
            squares = times(moves, [spread(m) for m in moves])
        else:
            moves = times(results, [spread(r) for r in rest])
            spreads = [spread(r) for r in results]
            squares = times(moves, [spread(m) for m in moves])
            first = [r - p for r, p in zip(results, times(moves, spreads))]
        second = times(squares, [spread(q) for q in first])
        results = [q + p for q, p in zip(first, second)]
    return results


def pack(low):
    lane = iota((64, LANES), 1) < 64
    tiles = []
    for t in range(2):
        tile = low[LANES * t : LANES * t + LANES, LANES * t : LANES * t + LANES]
        tiles.append(jnp.where(lane, tile[:64], tile[64:]))
    return jnp.concatenate(tiles, axis=1)


def unpack(packed):
    lanes = blocks_apart()
    return jnp.concatenate([packed * mask.astype(F32) for mask in lanes], axis=0)


def widened(results, lows, width, times):
    i, j = iota((CHUNK, CHUNK), 0), iota((CHUNK, CHUNK), 1)
    wide = times * width
    coupled = (i // wide == j // wide) & (i // width != j // width)
    half = [r.astype(BF16) for r in results]
    moves = [
        dot(r, jnp.where(coupled, low, 0.0).astype(BF16)).astype(BF16)
        for r, low in zip(half, lows)
    ]
    squares = [dot(m, m).astype(BF16) for m in moves] if times == 4 else None
    first = [r - dot(m, h) for r, m, h in zip(results, moves, half)]
    if times == 2:
        return first
    return [q + dot(m, q.astype(BF16)) for q, m in zip(first, squares)]


class Order:
    def __init__(self, n):
        self.away = iota((n, n), 0) - iota((n, n), 1)
        self.same = jnp.where(self.away == 0, 1.0, 0.0).astype(BF16)
        self.upto = [
            jnp.where(a >= 0, 1.0, 0.0).astype(BF16) for a in (self.away, -self.away)
        ]

    def block(self, key, rows):
        n = key.shape[0]
        pairs = dot(key, key, ((1,), (1,)))
        rows32 = rows.astype(F32)
        key32 = key.astype(F32)

        def down_columns(matrix, at):
            two = [jnp.broadcast_to(rows32[r : r + 1], (LANES, n)) for r in (at, at + 1)]
            both = dot(matrix, jnp.concatenate(two, axis=0).astype(BF16), ((1,), (1,)))
            return both[:, :LANES] + both[:, LANES:]

        wide = lambda v: jnp.concatenate([v] * (n // LANES), axis=1)
        found = []
        for d in range(2):
            down = down_columns(self.upto[d], 4 * d)
            beta = down_columns(self.same, 4 * d + 2)
            across = dot(rows, self.upto[1 - d])
            along = across[4 * d : 4 * d + 1] + across[4 * d + 1 : 4 * d + 2]
            reach = self.away if d == 0 else -self.away
            weights = jnp.where(
                reach >= 0, jnp.exp(jnp.where(reach >= 0, wide(down) - along, 0.0)), 0.0
            )
            total = down[n - 1 : n] if d == 0 else down[0:1]
            low = jnp.where(reach > 0, pairs * weights * wide(beta), 0.0)
            kept = (key32 * jnp.exp(total - down)).astype(BF16)
            found.append((low, beta, jnp.exp(down), kept, jnp.exp(total), weights))
        return found


def small_rows(got):
    low_lanes = iota((8, LANES), 1) < 64
    small = [got[p, S_AT:X_ROWS, :].astype(F32) for p in range(4)]
    first = [s[:8] for s in small]
    second = [s[8:] for s in small]
    turn = lambda v: pltpu.roll(v, 64, 1)
    blocks = [
        first[0],
        jnp.where(low_lanes, second[0], turn(first[1])),
        jnp.where(low_lanes, turn(first[1]), turn(second[1])),
        first[2],
        jnp.where(low_lanes, second[2], turn(first[3])),
        jnp.where(low_lanes, turn(first[3]), turn(second[3])),
    ]
    lane = iota((8, LANES), 1)
    ctx_small = jnp.zeros((8, LANES), F32)
    for p in range(4):
        here = (lane >= 8 * p) & (lane < 8 * p + 8)
        ctx_small = jnp.where(here, pltpu.roll(second[p], (64 + 8 * p) % 128, 1), ctx_small)
    rows = [
        jnp.concatenate([blocks[2 * m], blocks[2 * m + 1]], axis=1).astype(BF16)
        for m in range(CHUNKS)
    ]
    return rows, ctx_small


def latent_rows(got, at, m):
    pieces = {
        0: ((0, 0, 192), (1, 0, 64)),
        1: ((1, 64, 192), (2, 0, 128)),
        2: ((2, 128, 192), (3, 0, 192)),
    }[m]
    return jnp.concatenate([got[p, at + a : at + b, :] for p, a, b in pieces], axis=0)


def add_block(mine, so_far):
    nxt = dot(mine[:, HEAD:].astype(BF16), so_far.astype(BF16))
    return jnp.concatenate([nxt[:, :HEAD] + mine[:, :HEAD].astype(F32), nxt[:, HEAD:]], axis=1)


def token_maps(got, out, reads, offsets, weights_of, maps):
    order = Order(CHUNK)

    def ctx_rows(at):
        return jnp.concatenate(
            [got[p, at + SPAN : at + ROWS, :].astype(F32)[:CTX_OWN] for p in range(4)], axis=0
        )

    rows, ctx_small = small_rows(got)
    keys = [latent_rows(got, K_AT, m) for m in range(CHUNKS)]
    values = [latent_rows(got, V_AT, m).astype(F32) for m in range(CHUNKS)]
    ctx_key, ctx_value = ctx_rows(K_AT), ctx_rows(V_AT)
    padded = jnp.concatenate([ctx_key, jnp.zeros((LANES - 32, HEAD), F32)], axis=0).astype(BF16)
    ctx_lows = [f[0] for f in Order(LANES).block(padded, ctx_small.astype(BF16))]
    left = iota((64, LANES), 1) < 64
    ctx_low = jnp.concatenate(
        [
            jnp.where(left, ctx_lows[0][:64], pltpu.roll(ctx_lows[1][:64], 64, 1)),
            jnp.zeros((64, LANES), F32),
        ],
        axis=1,
    )
    lows, rights, kept, totals, decays = [], [], [], [], []
    for m in range(CHUNKS):
        for d, (low, beta, decayed, keep, total, weights) in enumerate(
            order.block(keys[m], rows[m])
        ):
            lows.append(low)
            key = keys[m].astype(F32) * (beta * decayed)
            rights.append(jnp.concatenate([values[m] * beta, key], axis=1).astype(BF16))
            kept.append(keep)
            totals.append(total)
            decays.append(decayed)
            weights_of[2 * m + d] = weights
    packed = packed_inverses([pack(low) for low in lows] + [ctx_low])
    inverses = widened([unpack(p) for p in packed[:-1]], lows, 64, 4)
    factors = [dot(t.astype(BF16), r).astype(BF16) for t, r in zip(inverses, rights)]
    unit = jnp.where(iota((HEAD, HEAD), 0) == iota((HEAD, HEAD), 1), 1.0, 0.0)
    for n in range(2 * CHUNKS):
        both = dot(kept[n], factors[n], ((0,), (0,)))
        maps[n] = jnp.concatenate([both[:, :HEAD], totals[n] * unit - both[:, HEAD:]], axis=1)

    so_far = [None, None]
    passed = [[None] * CHUNKS for _ in range(2)]
    for step in range(CHUNKS):
        for d in range(2):
            m = step if d == 0 else CHUNKS - 1 - step
            passed[d][m] = so_far[d]
            mine = maps[2 * m + d]
            so_far[d] = mine if step == 0 else add_block(mine, so_far[d])
    for m in range(CHUNKS):
        query = latent_rows(got, Q_AT, m)
        pairs = dot(query, keys[m], ((1,), (1,)))
        at = slice(m * CHUNK, (m + 1) * CHUNK)
        offset = None
        for d in range(2):
            n = 2 * m + d
            local = dot((pairs * weights_of[n]).astype(BF16), factors[n])
            read = (query.astype(F32) * decays[n] - local[:, HEAD:]).astype(BF16)
            mine = local[:, :HEAD]
            if passed[d][m] is not None:
                moved = dot(read, passed[d][m].astype(BF16))
                read, mine = moved[:, HEAD:].astype(BF16), mine + moved[:, :HEAD]
            reads[at, d * HEAD : (d + 1) * HEAD] = read
            offset = mine if offset is None else offset + mine
        offsets[at, :] = offset

    ctx_inverse = packed[-1][:32, :LANES]
    merged = ctx_inverse + pltpu.roll(ctx_inverse, 64, 1)
    merged = merged - jnp.where(iota((32, LANES), 0) == iota((32, LANES), 1), 1.0, 0.0)
    narrow = iota((16, LANES), 1) < 96
    turn = lambda v: pltpu.roll(v, 64, 1)
    spare = jnp.concatenate(
        [
            turn(ctx_key), ctx_key, turn(ctx_value), turn(ctx_small),
            jnp.where(narrow, turn(merged[:16]), pltpu.roll(merged[16:], 96, 1)),
            jnp.zeros((8, LANES), F32),
        ],
        axis=0,
    )
    left = iota((HEAD, LANES), 1) < 64
    whole = [
        jnp.concatenate([jnp.where(left, m[:, :HEAD], spare), m[:, HEAD:]], axis=1) for m in so_far
    ]
    place = lax.axis_index("z")
    for k in range(out.shape[0]):
        out[k] = jnp.where(k > place, whole[0], whole[1]).astype(BF16)


def read_states(got, reads, offsets, sent, out):
    count = got.shape[0]
    place = lax.axis_index("z")
    turn = lambda v: pltpu.roll(v, 64, 1)
    unit = jnp.where(iota((HEAD, HEAD), 0) == iota((HEAD, HEAD), 1), 1.0, 0.0)
    left = iota((32, LANES), 1) < 64
    lane = iota((16, LANES), 1)
    key, value, starts = [], [], []
    rows = [jnp.zeros((8, LANES), F32)] * 2
    none = jnp.zeros((16, LANES), F32)
    for k in range(count):
        spare = got[k, :, :LANES].astype(F32)
        key.append(jnp.where(left, turn(spare[:32]), spare[32:64]))
        value.append(turn(spare[64:96]))
        here = lane // 32 == k % 4
        at = 32 * (k % 4)
        rows[k // 4] = jnp.where(
            here[:8], pltpu.roll(spare[96:104], (at - 64) % LANES, 1), rows[k // 4]
        )
        for shift in (64, 96):
            one = jnp.where(here, pltpu.roll(spare[104:120], (at - shift) % LANES, 1), 0.0)
            starts.append(jnp.concatenate([one, none] if k < 4 else [none, one], axis=1))
    key = jnp.concatenate(key, axis=0).astype(BF16)
    value = jnp.concatenate(value, axis=0)
    start = jnp.concatenate(starts, axis=0)
    order = Order(CHUNK)
    found = order.block(key, jnp.concatenate(rows, axis=1).astype(BF16))
    lows = [f[0] for f in found]
    whole = jnp.where(order.away == 0, 1.0, 0.0)
    results = [jnp.where(a > 0, start, whole) for a in (order.away, -order.away)]
    inverses = widened(widened(results, lows, 32, 4), lows, 128, 2)
    ctx_states = []
    for inverse, (_, beta, _, kept, _, _) in zip(inverses, found):
        fresh = dot(inverse.astype(BF16), (value * beta).astype(BF16))
        ctx_states.append(dot(kept, fresh.astype(BF16), ((0,), (0,))))

    chains = [jnp.concatenate([jnp.zeros((HEAD, HEAD), F32), unit], axis=1)] * 2
    for step in range(count - 1):
        for d in range(2):
            k = step if d == 0 else count - 1 - step
            used = k < place if d == 0 else k > place
            chains[d] = jnp.where(used, add_block(got[k], chains[d]), chains[d])
    states = [
        (dot(c[:, HEAD:].astype(BF16), s.astype(BF16)) + c[:, :HEAD]).astype(BF16)
        for c, s in zip(chains, ctx_states)
    ]
    state = jnp.concatenate(states, axis=0)
    left = iota((48, LANES), 1) < 64
    for x in range(4):
        at = slice(SPAN * x, SPAN * x + SPAN)
        o = dot(reads[at, :], state) + offsets[at, :]
        gates = sent[x, V_AT : V_AT + SPAN, :].astype(F32)
        for y in range(4):
            own = slice(48 * y, 48 * y + 48)
            out[4 * x + y] = jnp.where(left, o[own], gates[own]).astype(BF16)


def mix(got, out_gain, gate, w_out, latent, out):
    left = iota((48, LANES), 1) < 64
    gain = out_gain[...].astype(F32)
    tiles = []
    for y in range(4):
        for h in range(2):
            one = got[8 * h + y].astype(F32)
            two = got[8 * h + 4 + y].astype(F32)
            o = jnp.where(left, one, pltpu.roll(two, 64, 1))
            gates = jnp.where(left, pltpu.roll(one, 64, 1), two)
            normed = o * lax.rsqrt(jnp.mean(o * o, axis=-1, keepdims=True) + NORM_EPS)
            tiles.append((normed * gain * gates).astype(BF16))
    gated = jnp.concatenate(tiles, axis=1)
    start = pl.multiple_of(lax.axis_index("tp") * 48, 16)
    own = latent[pl.ds(start, 48), :].astype(F32)
    for n in range(0, D, 512):
        mixed = dot(gated, w_out[:, n : n + 512])
        for c in range(0, 512, LANES):
            j = (n + c) // LANES
            cols = slice(n + c, n + c + LANES)
            out[:, cols] = (own[:, cols] + gate[j : j + 1, :] * mixed[:, c : c + LANES]).astype(BF16)


VM = pl.BlockSpec(memory_space=pltpu.VMEM)


HBM = pl.BlockSpec(memory_space=pltpu.HBM)


def call(body, name, n_in, outs, scratch=(), mib=16, n_hbm=0, flops=None):
    many = isinstance(outs, (list, tuple))
    return pl.pallas_call(
        body,
        out_shape=outs,
        in_specs=[VM] * n_in + [HBM] * n_hbm,
        out_specs=[VM] * len(outs) if many else VM,
        scratch_shapes=list(scratch),
        cost_estimate=flops and pl.CostEstimate(flops, 0, 0),
        compiler_params=pltpu.CompilerParams(vmem_limit_bytes=mib << 20),
        name=name,
    )


def shape(dims, dtype=BF16):
    return jax.ShapeDtypeStruct(dims, dtype)


def in_hbm(array):
    return pltpu.with_memory_space_constraint(array, pltpu.HBM)


def swap(array, axes):
    return lax.all_to_all(array, axes, 0, 0, tiled=True)


def on_device(
    latent, cond, context, ctx_cond, w_mod, norm_gain, w_query, w_key, w_value, w_outgate,
    w_decay, w_beta, decay_rate, decay_bias, extra_decay, out_gain, w_out,
):
    partial = call(
        partial_modulation, "partial_modulation", 0, shape((8, 24, LANES)),
        [
            pltpu.VMEM((24, LANES), F32), pltpu.VMEM(cond.shape, BF16),
            pltpu.VMEM(cond.shape, BF16), pltpu.VMEM(w_mod.shape, BF16),
            pltpu.SemaphoreType.DMA((3,)),
        ],
        16, 3, FLOPS,
    )(in_hbm(cond), in_hbm(ctx_cond[None, :]), in_hbm(w_mod))
    summed = call(
        sum_and_spread, "sum_and_spread", 1, shape((16, 24, LANES)), flops=FLOPS
    )(swap(partial, "z"))
    parts = swap(summed, ("x", "tp"))
    by_row = lambda w: w.transpose(1, 2, 0)
    sent, gate = call(
        project, "project", 13, [shape((4, X_ROWS, LANES)), shape((16, LANES), F32)],
        [pltpu.VMEM((96, LANES), F32), pltpu.VMEM((ROWS, D), BF16)],
    )(
        parts, norm_gain.reshape(16, LANES), latent, context, w_key, w_value, w_query, w_outgate,
        by_row(w_decay), by_row(w_beta), decay_rate, decay_bias, extra_decay,
    )
    held = swap(sent, "x")
    maps, reads, offsets = call(
        token_maps, "token_maps", 1,
        [shape((8, HEAD, 256)), shape((ROW_OF_X, 256)), shape((ROW_OF_X, HEAD), F32)],
        [
            pltpu.VMEM((2 * CHUNKS, CHUNK, CHUNK), F32), pltpu.VMEM((2 * CHUNKS, HEAD, 256), F32),
        ],
    )(held)
    reached = swap(maps, "z")
    outs = call(read_states, "read_states", 4, shape((16, 48, LANES)))(
        reached, reads, offsets, held
    )
    gathered = swap(outs, ("x", "tp"))
    mixed = call(mix, "mix", 5, shape((48, D)))(
        gathered, out_gain[None, :], gate, w_out, latent[0]
    )
    return mixed[None]


def solution(mesh):
    torus = Mesh(
        mesh.devices.reshape(8, 4, mesh.shape["tp"], mesh.shape["dp"]), ("z", "x", "tp", "dp")
    )
    sp = ("z", "x")
    return jax.shard_map(
        on_device,
        mesh=torus,
        in_specs=(
            P("dp", sp, None),
            P("dp", sp),
            P("dp", sp, None),
            P(sp),
            P(sp, "tp"),
            P(),
            P(None, "tp"),
            P(None, "tp"),
            P(None, "tp"),
            P(None, "tp"),
            P(None, None, "tp"),
            P(None, None, "tp"),
            P(None, "tp"),
            P(None, "tp"),
            P("dp", None, "tp", sp),
            P(),
            P(),
        ),
        out_specs=P("dp", ("z", "x", "tp"), None),
        check_vma=False,
    )
```

```python
import functools

import jax
import jax.numpy as jnp
from jax import lax
from jax.experimental import pallas as pl
from jax.experimental.pallas import tpu as pltpu
from jax.sharding import Mesh
from jax.sharding import PartitionSpec as P

D = 2048
HEAD = 128
LANES = 128
NORM_EPS = 1e-06
BETA_SCALE = 30.0

SPAN = 192
CTX_OWN = 8
ROWS = 208
CHUNK = 256
CHUNKS = 3
ROW_OF_X = 4 * SPAN

K_AT, V_AT, Q_AT, S_AT, X_ROWS = 0, 208, 416, 608, 624

FLOPS = 10**10

F32 = jnp.float32
BF16 = jnp.bfloat16


def dot(a, b, dims=((1,), (0,))):
    return lax.dot_general(a, b, (dims, ((), ())), preferred_element_type=F32)


def silu(v):
    return v / (1.0 + jnp.exp(-v))


def rounded(v):
    return v.astype(BF16).astype(F32)


def split_in_two(v):
    high = v.astype(BF16)
    return high.astype(F32), v - high.astype(F32)


def iota(shape, dim):
    return lax.broadcasted_iota(jnp.int32, shape, dim)


def fetch(pairs, sems):
    copies = [pltpu.make_async_copy(a, b, sems.at[n]) for n, (a, b) in enumerate(pairs)]
    for copy in copies:
        copy.start()
    return copies


def partial_modulation(cond_in, ctx_cond_in, w_mod_in, out, rows, cond, ctx_cond, w_mod, sems):
    pairs = ((w_mod_in, w_mod), (cond_in, cond), (ctx_cond_in, ctx_cond))
    for copy in fetch(pairs, sems):
        copy.wait()
    first = iota((8, cond.shape[1]), 0) == 0
    values = jnp.where(first, cond[...].astype(F32), ctx_cond[...].astype(F32))
    product = dot(silu(values).astype(BF16), w_mod[...])
    for r in range(2):
        for c in range(12):
            rows[r * 12 + c : r * 12 + c + 1, :] = product[r : r + 1, c * LANES : (c + 1) * LANES]
    value = rows[...].astype(BF16)
    for k in range(out.shape[0]):
        out[k] = value


def sum_and_spread(parts, out):
    total = parts[0].astype(F32)
    for k in range(1, parts.shape[0]):
        total = total + parts[k].astype(F32)
    value = total.astype(BF16)
    for k in range(out.shape[0]):
        out[k] = value


def project(
    parts, gain, latent, context, w_key, w_value, w_query, w_gate,
    w_decay, w_beta, rate_at, bias_at, extra, out, gate_out, mods, rows_in,
):
    for y in range(4):
        total = parts[y].astype(F32)
        for x in range(1, 4):
            total = total + parts[4 * x + y].astype(F32)
        mods[24 * y : 24 * y + 24, :] = total

    def row(which, block):
        at = (block // 12) * 24 + which * 12 + block % 12
        return mods[at : at + 1, :]

    for j in range(16):
        gate_out[j : j + 1, :] = row(0, 32 + j)

    def modulate(values, which, at):
        factor = lax.rsqrt(jnp.mean(values * values, axis=-1, keepdims=True) + NORM_EPS)
        for j in range(16):
            cols = slice(j * LANES, (j + 1) * LANES)
            scale = gain[j : j + 1, :].astype(F32) * (1.0 + row(which, 16 + j))
            tile = values[:, cols] * factor * scale + row(which, j)
            rows_in[at : at + values.shape[0], cols] = tile.astype(BF16)

    for g in range(0, SPAN, 64):
        modulate(latent[0, g : g + 64, :].astype(F32), 0, g)
    none = jnp.zeros((ROWS - SPAN - CTX_OWN, D), F32)
    modulate(jnp.concatenate([context[0].astype(F32), none], axis=0), 1, SPAN)
    inputs = rows_in[...]

    def heads(values):
        return [values[:, h * HEAD : (h + 1) * HEAD] for h in range(2)]

    def unit(v):
        return v * lax.rsqrt(jnp.sum(v * v, axis=-1, keepdims=True) + NORM_EPS)

    keys = heads(silu(rounded(dot(inputs, w_key[...]))))
    values = heads(silu(rounded(dot(inputs, w_value[...]))))
    queries = heads(silu(rounded(dot(inputs[:SPAN], w_query[...]))))
    gates = heads(silu(rounded(dot(inputs[:SPAN], w_gate[...]))))
    def column(at):
        row = iota((4, 1), 0)
        one = jnp.where(row == 0, at[0:1, 0:1], at[0:1, 1:2])
        two = jnp.where(row == 2, at[1:2, 0:1], at[1:2, 1:2])
        return jnp.where(row < 2, one, two)

    rate, bias = column(rate_at), column(bias_at)
    w_small = jnp.concatenate(
        [w[d].astype(F32) for w in (w_decay, w_beta) for d in range(2)], axis=0
    ).astype(BF16)
    latent_only = jnp.concatenate([extra[0, 0], extra[0, 1]], axis=0)
    added = jnp.concatenate([latent_only, jnp.zeros((4, ROWS - SPAN), F32)], axis=1)
    small = rounded(dot(w_small, inputs, ((1,), (1,))))
    decay_raw, beta_raw = small[:4], small[4:]
    pre = decay_raw + bias
    soft = jnp.maximum(pre, 0.0) + jnp.log1p(jnp.exp(-jnp.abs(pre)))
    log_decay = -rate * soft + added
    beta = BETA_SCALE * rate / (1.0 + jnp.exp(-beta_raw))
    pad = jnp.zeros((4, 256 - ROWS), F32)
    g_high, g_low = split_in_two(jnp.concatenate([log_decay, pad], axis=1))
    b_high, b_low = split_in_two(jnp.concatenate([beta, pad], axis=1))

    low_lanes = iota((ROWS, LANES), 1) < 64
    for h in range(2):
        key = unit(keys[h]).astype(BF16)
        query = (unit(queries[h]) * HEAD**-0.5).astype(BF16)
        gate = jnp.concatenate([gates[h], jnp.zeros((ROWS - SPAN, HEAD), F32)], axis=0)
        small_parts = [v[2 * d + h : 2 * d + h + 1] for d in range(2)
                       for v in (g_high, g_low, b_high, b_low)]
        eight = jnp.concatenate(small_parts, axis=0)
        eight = jnp.concatenate([eight[:, :LANES], eight[:, LANES:]], axis=0).astype(BF16)
        for half in range(2):
            peer = 2 * h + half
            out[peer, K_AT:V_AT, :] = key
            if half == 0:
                both = jnp.where(low_lanes, values[h], pltpu.roll(gate, 64, 1))
            else:
                both = jnp.where(low_lanes, pltpu.roll(values[h], 64, 1), gate)
            out[peer, V_AT:Q_AT, :] = both.astype(BF16)
            out[peer, Q_AT:S_AT, :] = query
            out[peer, S_AT:X_ROWS, :] = eight


def blocks_apart():
    lane = iota((64, 256), 1) // 64
    return [jnp.where(lane == b, 1.0, 0.0).astype(BF16) for b in range(4)]


def packed_inverses(lows):
    i, j = iota((64, 256), 0), iota((64, 256), 1) % 64
    lanes = blocks_apart()

    def spread(x):
        x = x.astype(BF16)
        return jnp.concatenate([x * mask for mask in lanes], axis=0)

    def times(xs, ys):
        return [dot(x.astype(BF16), y) for x, y in zip(xs, ys)]

    results = None
    for width in (1, 4, 16):
        coupled = (i // (4 * width) == j // (4 * width)) & (i // width != j // width)
        rest = [jnp.where(coupled, low, 0.0) for low in lows]
        if results is None:
            unit = jnp.where(i == j, 1.0, 0.0)
            moves = rest
            first = [unit - m for m in moves]
            squares = times(moves, [spread(m) for m in moves])
        else:
            moves = times(results, [spread(r) for r in rest])
            spreads = [spread(r) for r in results]
            squares = times(moves, [spread(m) for m in moves])
            first = [r - p for r, p in zip(results, times(moves, spreads))]
        second = times(squares, [spread(q) for q in first])
        results = [q + p for q, p in zip(first, second)]
    return results


def pack(low):
    lane = iota((64, LANES), 1) < 64
    tiles = []
    for t in range(2):
        tile = low[LANES * t : LANES * t + LANES, LANES * t : LANES * t + LANES]
        tiles.append(jnp.where(lane, tile[:64], tile[64:]))
    return jnp.concatenate(tiles, axis=1)


def unpack(packed):
    lanes = blocks_apart()
    return jnp.concatenate([packed * mask.astype(F32) for mask in lanes], axis=0)


def widened(results, lows, width, times):
    i, j = iota((CHUNK, CHUNK), 0), iota((CHUNK, CHUNK), 1)
    wide = times * width
    coupled = (i // wide == j // wide) & (i // width != j // width)
    half = [r.astype(BF16) for r in results]
    moves = [
        dot(r, jnp.where(coupled, low, 0.0).astype(BF16)).astype(BF16)
        for r, low in zip(half, lows)
    ]
    squares = [dot(m, m).astype(BF16) for m in moves] if times == 4 else None
    first = [r - dot(m, h) for r, m, h in zip(results, moves, half)]
    if times == 2:
        return first
    return [q + dot(m, q.astype(BF16)) for q, m in zip(first, squares)]


class Order:
    def __init__(self, n):
        self.away = iota((n, n), 0) - iota((n, n), 1)
        self.same = jnp.where(self.away == 0, 1.0, 0.0).astype(BF16)
        self.upto = [
            jnp.where(a >= 0, 1.0, 0.0).astype(BF16) for a in (self.away, -self.away)
        ]

    def block(self, key, rows):
        n = key.shape[0]
        pairs = dot(key, key, ((1,), (1,)))
        rows32 = rows.astype(F32)
        key32 = key.astype(F32)

        def down_columns(matrix, at):
            two = [jnp.broadcast_to(rows32[r : r + 1], (LANES, n)) for r in (at, at + 1)]
            both = dot(matrix, jnp.concatenate(two, axis=0).astype(BF16), ((1,), (1,)))
            return both[:, :LANES] + both[:, LANES:]

        wide = lambda v: jnp.concatenate([v] * (n // LANES), axis=1)
        found = []
        for d in range(2):
            down = down_columns(self.upto[d], 4 * d)
            beta = down_columns(self.same, 4 * d + 2)
            across = dot(rows, self.upto[1 - d])
            along = across[4 * d : 4 * d + 1] + across[4 * d + 1 : 4 * d + 2]
            reach = self.away if d == 0 else -self.away
            weights = jnp.where(
                reach >= 0, jnp.exp(jnp.where(reach >= 0, wide(down) - along, 0.0)), 0.0
            )
            total = down[n - 1 : n] if d == 0 else down[0:1]
            low = jnp.where(reach > 0, pairs * weights * wide(beta), 0.0)
            kept = (key32 * jnp.exp(total - down)).astype(BF16)
            found.append((low, beta, jnp.exp(down), kept, jnp.exp(total), weights))
        return found


def small_rows(got):
    low_lanes = iota((8, LANES), 1) < 64
    small = [got[p, S_AT:X_ROWS, :].astype(F32) for p in range(4)]
    first = [s[:8] for s in small]
    second = [s[8:] for s in small]
    turn = lambda v: pltpu.roll(v, 64, 1)
    blocks = [
        first[0],
        jnp.where(low_lanes, second[0], turn(first[1])),
        jnp.where(low_lanes, turn(first[1]), turn(second[1])),
        first[2],
        jnp.where(low_lanes, second[2], turn(first[3])),
        jnp.where(low_lanes, turn(first[3]), turn(second[3])),
    ]
    lane = iota((8, LANES), 1)
    ctx_small = jnp.zeros((8, LANES), F32)
    for p in range(4):
        here = (lane >= 8 * p) & (lane < 8 * p + 8)
        ctx_small = jnp.where(here, pltpu.roll(second[p], (64 + 8 * p) % 128, 1), ctx_small)
    rows = [
        jnp.concatenate([blocks[2 * m], blocks[2 * m + 1]], axis=1).astype(BF16)
        for m in range(CHUNKS)
    ]
    return rows, ctx_small


def latent_rows(got, at, m):
    pieces = {
        0: ((0, 0, 192), (1, 0, 64)),
        1: ((1, 64, 192), (2, 0, 128)),
        2: ((2, 128, 192), (3, 0, 192)),
    }[m]
    return jnp.concatenate([got[p, at + a : at + b, :] for p, a, b in pieces], axis=0)


def add_block(mine, so_far):
    nxt = dot(mine[:, HEAD:].astype(BF16), so_far.astype(BF16))
    return jnp.concatenate([nxt[:, :HEAD] + mine[:, :HEAD].astype(F32), nxt[:, HEAD:]], axis=1)


def token_maps(got, out, reads, offsets, weights_of, maps):
    order = Order(CHUNK)

    def ctx_rows(at):
        return jnp.concatenate(
            [got[p, at + SPAN : at + ROWS, :].astype(F32)[:CTX_OWN] for p in range(4)], axis=0
        )

    rows, ctx_small = small_rows(got)
    keys = [latent_rows(got, K_AT, m) for m in range(CHUNKS)]
    values = [latent_rows(got, V_AT, m).astype(F32) for m in range(CHUNKS)]
    ctx_key, ctx_value = ctx_rows(K_AT), ctx_rows(V_AT)
    padded = jnp.concatenate([ctx_key, jnp.zeros((LANES - 32, HEAD), F32)], axis=0).astype(BF16)
    ctx_lows = [f[0] for f in Order(LANES).block(padded, ctx_small.astype(BF16))]
    left = iota((64, LANES), 1) < 64
    ctx_low = jnp.concatenate(
        [
            jnp.where(left, ctx_lows[0][:64], pltpu.roll(ctx_lows[1][:64], 64, 1)),
            jnp.zeros((64, LANES), F32),
        ],
        axis=1,
    )
    lows, rights, kept, totals, decays = [], [], [], [], []
    for m in range(CHUNKS):
        for d, (low, beta, decayed, keep, total, weights) in enumerate(
            order.block(keys[m], rows[m])
        ):
            lows.append(low)
            key = keys[m].astype(F32) * (beta * decayed)
            rights.append(jnp.concatenate([values[m] * beta, key], axis=1).astype(BF16))
            kept.append(keep)
            totals.append(total)
            decays.append(decayed)
            weights_of[2 * m + d] = weights
    packed = packed_inverses([pack(low) for low in lows] + [ctx_low])
    inverses = widened([unpack(p) for p in packed[:-1]], lows, 64, 4)
    factors = [dot(t.astype(BF16), r).astype(BF16) for t, r in zip(inverses, rights)]
    unit = jnp.where(iota((HEAD, HEAD), 0) == iota((HEAD, HEAD), 1), 1.0, 0.0)
    for n in range(2 * CHUNKS):
        both = dot(kept[n], factors[n], ((0,), (0,)))
        maps[n] = jnp.concatenate([both[:, :HEAD], totals[n] * unit - both[:, HEAD:]], axis=1)

    so_far = [None, None]
    passed = [[None] * CHUNKS for _ in range(2)]
    for step in range(CHUNKS):
        for d in range(2):
            m = step if d == 0 else CHUNKS - 1 - step
            passed[d][m] = so_far[d]
            mine = maps[2 * m + d]
            so_far[d] = mine if step == 0 else add_block(mine, so_far[d])
    for m in range(CHUNKS):
        query = latent_rows(got, Q_AT, m)
        pairs = dot(query, keys[m], ((1,), (1,)))
        at = slice(m * CHUNK, (m + 1) * CHUNK)
        offset = None
        for d in range(2):
            n = 2 * m + d
            local = dot((pairs * weights_of[n]).astype(BF16), factors[n])
            read = (query.astype(F32) * decays[n] - local[:, HEAD:]).astype(BF16)
            mine = local[:, :HEAD]
            if passed[d][m] is not None:
                moved = dot(read, passed[d][m].astype(BF16))
                read, mine = moved[:, HEAD:].astype(BF16), mine + moved[:, :HEAD]
            reads[at, d * HEAD : (d + 1) * HEAD] = read
            offset = mine if offset is None else offset + mine
        offsets[at, :] = offset

    ctx_inverse = packed[-1][:32, :LANES]
    merged = ctx_inverse + pltpu.roll(ctx_inverse, 64, 1)
    merged = merged - jnp.where(iota((32, LANES), 0) == iota((32, LANES), 1), 1.0, 0.0)
    narrow = iota((16, LANES), 1) < 96
    turn = lambda v: pltpu.roll(v, 64, 1)
    spare = jnp.concatenate(
        [
            turn(ctx_key), ctx_key, turn(ctx_value), turn(ctx_small),
            jnp.where(narrow, turn(merged[:16]), pltpu.roll(merged[16:], 96, 1)),
            jnp.zeros((8, LANES), F32),
        ],
        axis=0,
    )
    left = iota((HEAD, LANES), 1) < 64
    whole = [
        jnp.concatenate([jnp.where(left, m[:, :HEAD], spare), m[:, HEAD:]], axis=1) for m in so_far
    ]
    place = lax.axis_index("z")
    for k in range(out.shape[0]):
        out[k] = jnp.where(k > place, whole[0], whole[1]).astype(BF16)


def read_states(got, reads, offsets, sent, out):
    count = got.shape[0]
    place = lax.axis_index("z")
    turn = lambda v: pltpu.roll(v, 64, 1)
    unit = jnp.where(iota((HEAD, HEAD), 0) == iota((HEAD, HEAD), 1), 1.0, 0.0)
    left = iota((32, LANES), 1) < 64
    lane = iota((16, LANES), 1)
    key, value, starts = [], [], []
    rows = [jnp.zeros((8, LANES), F32)] * 2
    none = jnp.zeros((16, LANES), F32)
    for k in range(count):
        spare = got[k, :, :LANES].astype(F32)
        key.append(jnp.where(left, turn(spare[:32]), spare[32:64]))
        value.append(turn(spare[64:96]))
        here = lane // 32 == k % 4
        at = 32 * (k % 4)
        rows[k // 4] = jnp.where(
            here[:8], pltpu.roll(spare[96:104], (at - 64) % LANES, 1), rows[k // 4]
        )
        for shift in (64, 96):
            one = jnp.where(here, pltpu.roll(spare[104:120], (at - shift) % LANES, 1), 0.0)
            starts.append(jnp.concatenate([one, none] if k < 4 else [none, one], axis=1))
    key = jnp.concatenate(key, axis=0).astype(BF16)
    value = jnp.concatenate(value, axis=0)
    start = jnp.concatenate(starts, axis=0)
    order = Order(CHUNK)
    found = order.block(key, jnp.concatenate(rows, axis=1).astype(BF16))
    lows = [f[0] for f in found]
    whole = jnp.where(order.away == 0, 1.0, 0.0)
    results = [jnp.where(a > 0, start, whole) for a in (order.away, -order.away)]
    inverses = widened(widened(results, lows, 32, 4), lows, 128, 2)
    ctx_states = []
    for inverse, (_, beta, _, kept, _, _) in zip(inverses, found):
        fresh = dot(inverse.astype(BF16), (value * beta).astype(BF16))
        ctx_states.append(dot(kept, fresh.astype(BF16), ((0,), (0,))))

    chains = [jnp.concatenate([jnp.zeros((HEAD, HEAD), F32), unit], axis=1)] * 2
    for step in range(count - 1):
        for d in range(2):
            k = step if d == 0 else count - 1 - step
            used = k < place if d == 0 else k > place
            chains[d] = jnp.where(used, add_block(got[k], chains[d]), chains[d])
    states = [
        (dot(c[:, HEAD:].astype(BF16), s.astype(BF16)) + c[:, :HEAD]).astype(BF16)
        for c, s in zip(chains, ctx_states)
    ]
    state = jnp.concatenate(states, axis=0)
    left = iota((48, LANES), 1) < 64
    for x in range(4):
        at = slice(SPAN * x, SPAN * x + SPAN)
        o = dot(reads[at, :], state) + offsets[at, :]
        gates = sent[x, V_AT : V_AT + SPAN, :].astype(F32)
        for y in range(4):
            own = slice(48 * y, 48 * y + 48)
            out[4 * x + y] = jnp.where(left, o[own], gates[own]).astype(BF16)


def mix(got, out_gain, gate, w_out, latent, out_at, out, sems):
    left = iota((48, LANES), 1) < 64
    gain = out_gain[...].astype(F32)
    tiles = []
    for y in range(4):
        for h in range(2):
            one = got[8 * h + y].astype(F32)
            two = got[8 * h + 4 + y].astype(F32)
            o = jnp.where(left, one, pltpu.roll(two, 64, 1))
            gates = jnp.where(left, pltpu.roll(one, 64, 1), two)
            normed = o * lax.rsqrt(jnp.mean(o * o, axis=-1, keepdims=True) + NORM_EPS)
            tiles.append((normed * gain * gates).astype(BF16))
    gated = jnp.concatenate(tiles, axis=1)
    start = pl.multiple_of(lax.axis_index("tp") * 48, 16)
    own = latent[pl.ds(start, 48), :].astype(F32)
    copies = []
    for n in range(0, D, 512):
        mixed = dot(gated, w_out[:, n : n + 512])
        for c in range(0, 512, LANES):
            j = (n + c) // LANES
            cols = slice(n + c, n + c + LANES)
            out[:, cols] = (own[:, cols] + gate[j : j + 1, :] * mixed[:, c : c + LANES]).astype(BF16)
        part = (slice(None), pl.ds(n, 512))
        copies.append(pltpu.make_async_copy(out.at[part], out_at.at[part], sems.at[n // 512]))
        copies[-1].start()
    for copy in copies:
        copy.wait()


VM = pl.BlockSpec(memory_space=pltpu.VMEM)


HBM = pl.BlockSpec(memory_space=pltpu.HBM)


def call(body, name, n_in, outs, scratch=(), mib=16, n_hbm=0, flops=None, out_space=VM):
    many = isinstance(outs, (list, tuple))
    return pl.pallas_call(
        body,
        out_shape=outs,
        in_specs=[VM] * n_in + [HBM] * n_hbm,
        out_specs=[VM] * len(outs) if many else out_space,
        scratch_shapes=list(scratch),
        cost_estimate=flops and pl.CostEstimate(flops, 0, 0),
        compiler_params=pltpu.CompilerParams(vmem_limit_bytes=mib << 20),
        name=name,
    )


def shape(dims, dtype=BF16):
    return jax.ShapeDtypeStruct(dims, dtype)


def in_hbm(array):
    return pltpu.with_memory_space_constraint(array, pltpu.HBM)


def swap(array, axes):
    return lax.all_to_all(array, axes, 0, 0, tiled=True)


def on_device(
    latent, cond, context, ctx_cond, w_mod, norm_gain, w_query, w_key, w_value, w_outgate,
    w_decay, w_beta, decay_rate, decay_bias, extra_decay, out_gain, w_out,
):
    partial = call(
        partial_modulation, "partial_modulation", 0, shape((8, 24, LANES)),
        [
            pltpu.VMEM((24, LANES), F32), pltpu.VMEM(cond.shape, BF16),
            pltpu.VMEM(cond.shape, BF16), pltpu.VMEM(w_mod.shape, BF16),
            pltpu.SemaphoreType.DMA((3,)),
        ],
        16, 3, FLOPS,
    )(in_hbm(cond), in_hbm(ctx_cond[None, :]), in_hbm(w_mod))
    summed = call(
        sum_and_spread, "sum_and_spread", 1, shape((16, 24, LANES)), flops=FLOPS
    )(swap(partial, "z"))
    parts = swap(summed, ("x", "tp"))
    by_row = lambda w: w.transpose(1, 2, 0)
    sent, gate = call(
        project, "project", 13, [shape((4, X_ROWS, LANES)), shape((16, LANES), F32)],
        [pltpu.VMEM((96, LANES), F32), pltpu.VMEM((ROWS, D), BF16)],
    )(
        parts, norm_gain.reshape(16, LANES), latent, context, w_key, w_value, w_query, w_outgate,
        by_row(w_decay), by_row(w_beta), decay_rate, decay_bias, extra_decay,
    )
    held = swap(sent, "x")
    maps, reads, offsets = call(
        token_maps, "token_maps", 1,
        [shape((8, HEAD, 256)), shape((ROW_OF_X, 256)), shape((ROW_OF_X, HEAD), F32)],
        [
            pltpu.VMEM((2 * CHUNKS, CHUNK, CHUNK), F32), pltpu.VMEM((2 * CHUNKS, HEAD, 256), F32),
        ],
    )(held)
    reached = swap(maps, "z")
    outs = call(read_states, "read_states", 4, shape((16, 48, LANES)))(
        reached, reads, offsets, held
    )
    gathered = swap(outs, ("x", "tp"))
    mixed = call(
        mix, "mix", 5, shape((48, D)),
        [pltpu.VMEM((48, D), BF16), pltpu.SemaphoreType.DMA((4,))], out_space=HBM,
    )(
        gathered, out_gain[None, :], gate, w_out, latent[0]
    )
    return mixed[None]


def solution(mesh):
    torus = Mesh(
        mesh.devices.reshape(8, 4, mesh.shape["tp"], mesh.shape["dp"]), ("z", "x", "tp", "dp")
    )
    sp = ("z", "x")
    return jax.shard_map(
        on_device,
        mesh=torus,
        in_specs=(
            P("dp", sp, None),
            P("dp", sp),
            P("dp", sp, None),
            P(sp),
            P(sp, "tp"),
            P(),
            P(None, "tp"),
            P(None, "tp"),
            P(None, "tp"),
            P(None, "tp"),
            P(None, None, "tp"),
            P(None, None, "tp"),
            P(None, "tp"),
            P(None, "tp"),
            P("dp", None, "tp", sp),
            P(),
            P(),
        ),
        out_specs=P("dp", ("z", "x", "tp"), None),
        check_vma=False,
    )
```
